512 devices in a mesh: sp: 32 (over z, core), tp: 16 (over y, x).
Axes of the slice: x: 4, y: 4, z: 16, core: 2. Of those that a mesh axis runs over, the one named last changes fastest.
Arguments:
- prompt: bfloat16 [32, 8192, 2048], P('tp', 'sp'), may hold values from -6 to 6
- input_gain: float32 [2048], replicated, may hold values from 0.1 to 1.9
- key_weight: bfloat16 [1024, 2048], P('tp'), may hold values from -0.125 to 0.125
- value_weight: bfloat16 [1024, 2048], P('tp'), may hold values from -0.125 to 0.125
- key_gain: float32 [64], replicated, may hold values from 0.1 to 1.9
- queries: bfloat16 [32, 2, 1024], P('sp', None, 'tp'), may hold values from -6 to 6
- score_bias: float32 [2, 16], replicated, may hold values from -9 to -2
Outputs:
- keys: bfloat16 [32, 1024, 8192], P('sp', 'tp')
- values: bfloat16 [32, 1024, 8192], P('sp', 'tp')
- first_read: bfloat16 [32, 2, 1024], P('sp', None, 'tp')
The draws below stay inside these ranges and needn't reach their ends.
All inputs are finite; a program needn't handle non-finite values.
Results may differ from the reference program's by a relative error of at most 0.01.
Values may be sent and summed in bfloat16 or wider, within the bound.
A program may use at most 64 MiB of HBM per device.

```python
import math
import jax
import jax.numpy as jnp
from jax import lax

D = 2048
KV_HEADS = 16
HEAD = 64
GROUP = 2
SEQS = 32
LEN = 8192
KVW = 1024


def shard_levels(key, extent, split, low, high):
    def one(position, blocks):
        draws = jax.random.uniform(jax.random.fold_in(jax.random.fold_in(key, 6), position), (blocks,), jnp.float32, low / len(split), high / len(split))
        return jnp.repeat(jnp.exp(draws), extent[position] // blocks).reshape((-1,) + (1,) * (len(extent) - position - 1))

    loudness = one(*split[0])
    for cut in split[1:]:
        loudness = loudness * one(*cut)
    return loudness


def gaussian(stream_key, dims, scale, reach, shards=(), held_as=jnp.bfloat16):
    array = jax.random.normal(stream_key, dims, jnp.float32) * scale
    if len(shards) > 0:
        array = shard_levels(stream_key, dims, shards, -0.22, 0.18) * array
    return jnp.clip(array, min=-reach, max=reach).astype(held_as)


def setup_inputs(seed: int = 0) -> dict:
    key_of = jax.random.split(jax.random.key(seed), 8)
    prompt = gaussian(key_of[0], (SEQS, LEN, D), 1.0, 6.0, ((0, 16), (1, 32)))
    input_gain = jnp.clip(1.0 + 0.18 * jax.random.normal(key_of[1], (D,), jnp.float32), 0.1, 1.9)
    key_weight = gaussian(key_of[2], (KVW, D), D ** -0.5, 0.125, ((0, 16),))
    value_weight = gaussian(key_of[3], (KVW, D), D ** -0.5, 0.125, ((0, 16),))
    key_gain = jnp.clip(1.0 + 0.18 * jax.random.normal(key_of[4], (HEAD,), jnp.float32), 0.1, 1.9)
    queries = gaussian(key_of[5], (SEQS, GROUP, KVW), 1.0, 6.0, ((0, 32), (2, 16)))
    score_bias = jnp.clip(jax.random.uniform(key_of[6], (GROUP, KV_HEADS), jnp.float32, -9.0, -2.0), -9.0, -2.0)
    return dict(prompt=prompt, input_gain=input_gain, key_weight=key_weight, value_weight=value_weight, key_gain=key_gain, queries=queries, score_bias=score_bias)


epsilon = 1e-06

def reference(prompt, input_gain, key_weight, value_weight, key_gain, queries, score_bias):

    def one_sequence(pair):
        rows, query = pair
        flat = rows.astype(jnp.float32)
        normed = (flat * lax.rsqrt(lax.optimization_barrier(jnp.mean(flat * flat, axis=-1, keepdims=True)) + epsilon) * input_gain).astype(jnp.bfloat16)
        key_raw = jnp.dot(normed, key_weight.T, preferred_element_type=jnp.float32).reshape(LEN, KV_HEADS, HEAD)
        key_norm = (key_raw * lax.rsqrt(lax.optimization_barrier(jnp.mean(key_raw * key_raw, axis=-1, keepdims=True)) + epsilon) * key_gain).astype(jnp.bfloat16)
        value_rows = jnp.dot(normed, value_weight.T, preferred_element_type=jnp.float32).astype(jnp.bfloat16)
        query_heads = query.astype(jnp.float32).reshape(GROUP, KV_HEADS, HEAD)
        scores = jnp.einsum('ghd,shd->ghs', query_heads, key_norm.astype(jnp.float32)) / math.sqrt(HEAD)
        scores = scores + score_bias[:, :, None]
        log_break = jax.nn.log_sigmoid(scores)
        log_keep = jax.nn.log_sigmoid(-scores)
        later = lax.cumsum(log_keep, axis=2, reverse=True) - log_keep
        weights = jnp.exp(log_break + later).astype(jnp.bfloat16)
        value_heads = value_rows.astype(jnp.float32).reshape(LEN, KV_HEADS, HEAD)
        read = jnp.einsum('ghs,shd->ghd', weights.astype(jnp.float32), value_heads).astype(jnp.bfloat16)
        return (key_norm.reshape(LEN, KVW).T, value_rows.T, read.reshape(GROUP, KVW))
    keys, values, first_read = lax.map(one_sequence, (prompt, queries))
    return (keys, values, first_read)
```

```python
import jax
import jax.numpy as jnp
from jax import lax
from jax.experimental import pallas as pl
from jax.experimental.pallas import tpu as pltpu
from jax.sharding import PartitionSpec as P

HEAD = 64
EPS = 1e-06
MESH = pl.DeviceIdType.MESH
Y, X, Z = 4, 4, 16
POS = 256
D = 2048

ORDER = [(0, 0), (1, 0), (3, 0), (0, 1), (0, 3), (2, 0), (0, 2),
         (1, 1), (1, 3), (3, 1), (3, 3), (2, 1), (2, 3), (1, 2), (3, 2), (2, 2)]
SLOT = {offset: slot for slot, offset in enumerate(ORDER)}
GROUPS = [(1, 5), (5, 7), (7, 11), (11, 15), (15, 16)]


def exchange(prompt, gain, kw, vw, kgain, kv, pbuf, nbuf, wbuf, sbuf, mbuf,
             lsem, ws, wr, fs, ps, pr, ms, mr, zs, zr):
    sp = lax.axis_index("sp")
    tp = lax.axis_index("tp")
    z, c = sp // 2, lax.rem(sp, 2)
    y, x = tp // X, lax.rem(tp, X)
    first = c == 0

    def plane(dy, dx):
        return lax.rem(y + dy + Y, Y) * X + lax.rem(x + dx + X, X)

    loads = [
        pltpu.make_async_copy(prompt.at[0], pbuf.at[0], lsem.at[0]),
        pltpu.make_async_copy(prompt.at[1], pbuf.at[1], lsem.at[1]),
        pltpu.make_async_copy(kw, wbuf.at[0, 0], lsem.at[2]),
        pltpu.make_async_copy(vw, wbuf.at[0, 1], lsem.at[3]),
    ]
    for load in loads:
        load.start()

    barrier = pltpu.get_barrier_semaphore()
    for dy, dx in ORDER[1:]:
        pl.semaphore_signal(barrier, inc=1, device_id=(sp, plane(dy, dx)), device_id_type=MESH)
    for step in range(1, 2 * Z):
        pl.semaphore_signal(barrier, inc=1, device_id=(lax.rem(sp + step, 2 * Z), tp), device_id_type=MESH)

    gain_row = gain[...]
    for parity in range(2):
        loads[parity].wait()

        @pl.loop(0, POS // 32)
        def _(step):
            rows = pl.ds(pl.multiple_of(step * 32, 32), 32)
            flat = pbuf[parity, rows, :].astype(jnp.float32)
            scale = lax.rsqrt(jnp.mean(flat * flat, axis=-1, keepdims=True) + EPS)
            nbuf[parity, rows, :] = (flat * scale * gain_row).astype(jnp.bfloat16)

    eye = lax.broadcasted_iota(jnp.int32, (HEAD, HEAD), 0) == lax.broadcasted_iota(jnp.int32, (HEAD, HEAD), 1)
    gain_col = jnp.sum(jnp.where(eye, kgain[...], 0.0), axis=1, keepdims=True)

    def project(lo, hi):
        count = hi - lo
        weights = wbuf[lo:hi].reshape(count * 2 * HEAD, D)
        for parity in range(2):
            raw = lax.dot_general(weights, nbuf[parity], (((1,), (1,)), ((), ())),
                                  preferred_element_type=jnp.float32)
            for i in range(count):
                key = raw[i * 2 * HEAD: i * 2 * HEAD + HEAD]
                scale = lax.rsqrt(jnp.mean(key * key, axis=0, keepdims=True) + EPS)
                sbuf[lo + i, parity, 0] = (key * scale * gain_col).astype(jnp.bfloat16)
                sbuf[lo + i, parity, 1] = raw[i * 2 * HEAD + HEAD: (i + 1) * 2 * HEAD].astype(jnp.bfloat16)

    loads[2].wait()
    loads[3].wait()
    project(0, 1)
    pl.semaphore_wait(barrier, 15 + 2 * Z - 1)

    def remote(src, dst, send, recv, device):
        return pltpu.make_async_remote_copy(src_ref=src, dst_ref=dst, send_sem=send, recv_sem=recv,
                                            device_id=device, device_id_type=MESH)

    sends = []

    for i, offset in enumerate(ORDER[1:7]):
        copy = remote(wbuf.at[0, c], wbuf.at[SLOT[offset], c], ws.at[i], wr.at[SLOT[offset]],
                      (sp, plane(-offset[0], -offset[1])))
        copy.start()
        sends.append(copy)

    columns = pl.ds(pl.multiple_of(sp * POS, POS), POS)

    def onward(slot):
        dy, dx = ORDER[slot]
        owner = plane(-dy, -dx)
        source = sbuf if slot == 0 else mbuf
        for parity in range(2):
            target = owner * 2 + parity
            far = remote(source.at[slot, parity], kv.at[:, :, columns], zs.at[slot, parity], zr.at[sp], (target, tp))
            near = pltpu.make_async_copy(source.at[slot, parity], kv.at[:, :, columns], zs.at[slot, parity])

            @pl.when(target != sp)
            def _():
                far.start()

            @pl.when(target == sp)
            def _():
                near.start()

    def finish(slot):
        dy, dx = ORDER[slot]
        owner = plane(-dy, -dx)
        source = sbuf if slot == 0 else mbuf
        for parity in range(2):
            target = owner * 2 + parity
            far = remote(source.at[slot, parity], kv.at[:, :, columns], zs.at[slot, parity], zr.at[sp], (target, tp))
            near = pltpu.make_async_copy(source.at[slot, parity], kv.at[:, :, columns], zs.at[slot, parity])

            @pl.when(target != sp)
            def _():
                far.wait_send()

            @pl.when(target == sp)
            def _():
                near.wait()

    onward(0)

    partner = (z * 2 + 1 - c, tp)

    def arrive(slot):
        half = remote(wbuf.at[slot, c], wbuf.at[slot, c], ps.at[slot], wr.at[slot], partner)
        half.wait_recv()
        over = remote(wbuf.at[slot, c], wbuf.at[slot, c], ps.at[slot], pr.at[slot], partner)
        over.start()
        sends.append(over)

    def other(slot):
        remote(wbuf.at[slot, 1 - c], wbuf.at[slot, 1 - c], ps.at[slot], pr.at[slot], partner).wait_recv()

    def spread(step):
        source = jnp.where(first, SLOT[(step, 0)], SLOT[(0, step)])
        for hop in (1, 3, 2):
            slot = jnp.where(first, SLOT[(step, hop)], SLOT[(hop, step)])
            target = jnp.where(first, plane(0, -hop), plane(-hop, 0))
            index = step * 4 + hop
            copy = remote(wbuf.at[source, c], wbuf.at[slot, c], fs.at[index], wr.at[slot], (sp, target))
            copy.start()
            sends.append(copy)

    def hand(slot):
        dy, dx = ORDER[slot]
        copy = remote(sbuf.at[slot], mbuf.at[slot], ms.at[slot], mr.at[slot], (sp, plane(dy, dx)))
        copy.start()
        sends.append(copy)

    def relay(slot):
        remote(sbuf.at[slot], mbuf.at[slot], ms.at[slot], mr.at[slot], (sp, tp)).wait_recv()
        onward(slot)

    for number, (lo, hi) in enumerate(GROUPS):
        for slot in range(lo, hi):
            arrive(slot)
        if number == 0:
            spread(1)
            spread(3)
        if number == 1:
            spread(2)
        for slot in range(lo, hi):
            other(slot)
        project(lo, hi)
        for slot in range(lo, hi):
            hand(slot)
        if number > 0:
            for slot in range(*GROUPS[number - 1]):
                relay(slot)
    for slot in range(*GROUPS[-1]):
        relay(slot)

    for copy in sends:
        copy.wait_send()
    for slot in range(16):
        finish(slot)

    @pl.loop(0, 2 * Z)
    def _(p):
        @pl.when(p != sp)
        def _():
            span = kv.at[:, :, pl.ds(pl.multiple_of(p * POS, POS), POS)]
            remote(span, span, zs.at[0, 0], zr.at[p], partner).wait_recv()


def read(kv, queries, bias, keys, values, out, kbuf, vbuf, lsem, ssem):
    length = kbuf.shape[1]
    head = lax.axis_index("tp")
    load_k = pltpu.make_async_copy(kv.at[0], kbuf, lsem.at[0])
    load_v = pltpu.make_async_copy(kv.at[1], vbuf, lsem.at[1])
    load_k.start()
    load_v.start()
    load_k.wait()
    store_k = pltpu.make_async_copy(kbuf, keys.at[0], ssem.at[0])
    store_k.start()
    q = jnp.concatenate([queries[0], jnp.zeros((6, HEAD), jnp.bfloat16)], axis=0)
    scores = jnp.dot(q, kbuf[...], preferred_element_type=jnp.float32) * 0.125
    row = lax.broadcasted_iota(jnp.int32, (8, 1), 0)
    scores = scores + jnp.where(row == 0, bias[0, head], bias[1, head])
    soft = jnp.log1p(jnp.exp(-jnp.abs(scores)))
    log_break = jnp.minimum(scores, 0.0) - soft
    log_keep = jnp.minimum(-scores, 0.0) - soft
    blocks = length // 128
    stacked = jnp.concatenate([log_keep[:, b * 128:(b + 1) * 128] for b in range(blocks)], axis=0)
    r = lax.broadcasted_iota(jnp.int32, (128, 256), 0)
    col = lax.broadcasted_iota(jnp.int32, (128, 256), 1)
    tri = jnp.where((r > col) | (col >= 128), 1.0, 0.0).astype(jnp.float32)
    sums = jnp.dot(stacked, tri, preferred_element_type=jnp.float32, precision=lax.Precision.HIGHEST)
    carry = jnp.zeros((8, 128), jnp.float32)
    parts = [None] * blocks
    for b in range(blocks - 1, -1, -1):
        parts[b] = sums[b * 8:(b + 1) * 8, :128] + carry
        carry = carry + sums[b * 8:(b + 1) * 8, 128:]
    later = jnp.concatenate(parts, axis=1)
    weights = jnp.exp(log_break + later).astype(jnp.bfloat16)
    load_v.wait()
    store_v = pltpu.make_async_copy(vbuf, values.at[0], ssem.at[1])
    store_v.start()
    result = lax.dot_general(weights, vbuf[...], (((1,), (1,)), ((), ())), preferred_element_type=jnp.float32)
    out[0] = result[:2].astype(jnp.bfloat16)
    store_k.wait()
    store_v.wait()


def local(prompt, input_gain, key_weight, value_weight, key_gain, queries, score_bias):
    hbm = pl.BlockSpec(memory_space=pltpu.HBM)
    vmem = pl.BlockSpec(memory_space=pltpu.VMEM)
    length = POS * 2 * Z
    dma = pltpu.SemaphoreType.DMA
    kv = pl.pallas_call(
        exchange,
        out_shape=jax.ShapeDtypeStruct((2, HEAD, length), jnp.bfloat16),
        in_specs=[hbm, vmem, hbm, hbm, vmem],
        out_specs=hbm,
        scratch_shapes=[
            pltpu.VMEM((2, POS, D), jnp.bfloat16),
            pltpu.VMEM((2, POS, D), jnp.bfloat16),
            pltpu.VMEM((16, 2, HEAD, D), jnp.bfloat16),
            pltpu.VMEM((16, 2, 2, HEAD, POS), jnp.bfloat16),
            pltpu.VMEM((16, 2, 2, HEAD, POS), jnp.bfloat16),
            dma((4,)), dma((6,)), dma((16,)), dma((16,)), dma((16,)), dma((16,)),
            dma((16,)), dma((16,)), dma((16, 2)), dma((32,)),
        ],
        compiler_params=pltpu.CompilerParams(collective_id=0, has_side_effects=True),
        name="exchange",
    )(prompt, input_gain.reshape(1, D), key_weight, value_weight, key_gain.reshape(1, HEAD))
    keys, values, out = pl.pallas_call(
        read,
        out_shape=(
            jax.ShapeDtypeStruct((1, HEAD, length), jnp.bfloat16),
            jax.ShapeDtypeStruct((1, HEAD, length), jnp.bfloat16),
            jax.ShapeDtypeStruct((1, 2, HEAD), jnp.bfloat16),
        ),
        in_specs=[hbm, vmem, pl.BlockSpec(memory_space=pltpu.SMEM)],
        out_specs=(hbm, hbm, vmem),
        scratch_shapes=[
            pltpu.VMEM((HEAD, length), jnp.bfloat16),
            pltpu.VMEM((HEAD, length), jnp.bfloat16),
            dma((2,)), dma((2,)),
        ],
        name="read",
    )(kv, queries, score_bias)
    return keys, values, out


def solution(mesh):
    placed = (P("tp", "sp", None), P(), P("tp", None), P("tp", None), P(), P("sp", None, "tp"), P())
    return jax.shard_map(
        local,
        mesh=mesh,
        in_specs=placed,
        out_specs=(P("sp", "tp", None), P("sp", "tp", None), P("sp", None, "tp")),
        check_vma=False,
    )
```

```python
import jax
import jax.numpy as jnp
from jax import lax
from jax.experimental import pallas as pl
from jax.experimental.pallas import tpu as pltpu
from jax.sharding import PartitionSpec as P

HEAD = 64
EPS = 1e-06
MESH = pl.DeviceIdType.MESH
Y, X, Z = 4, 4, 16
POS = 256
D = 2048

ORDER = [(0, 0), (1, 0), (3, 0), (0, 1), (0, 3), (2, 0), (0, 2),
         (1, 1), (1, 3), (3, 1), (3, 3), (2, 1), (2, 3), (1, 2), (3, 2), (2, 2)]
SLOT = {offset: slot for slot, offset in enumerate(ORDER)}
UNIT = 16
STEPS = [8, 7, -7, 6, -6, 5, -5, 4, -4, 3, -3, 2, -2, 1, -1, 0]
GROUPS = [(1, 5), (5, 7), (7, 11), (11, 15), (15, 16)]


def exchange(prompt, gain, kw, vw, kgain, kv, pbuf, nbuf, ubuf, xbuf, wbuf, sbuf, mbuf, ybuf, tbuf, kvbuf,
             lsem, us, ur, bs, br, ws, wr, fs, ps, pr, ms, mr, zs, zr, ys, yr):
    sp = lax.axis_index("sp")
    tp = lax.axis_index("tp")
    z, c = sp // 2, lax.rem(sp, 2)
    y, x = tp // X, lax.rem(tp, X)
    first = c == 0
    partner = (z * 2 + 1 - c, tp)

    def plane(dy, dx):
        return lax.rem(y + dy + Y, Y) * X + lax.rem(x + dx + X, X)

    def remote(src, dst, send, recv, device):
        return pltpu.make_async_remote_copy(src_ref=src, dst_ref=dst, send_sem=send, recv_sem=recv,
                                            device_id=device, device_id_type=MESH)

    loads = [
        pltpu.make_async_copy(prompt.at[0], pbuf.at[0], lsem.at[0]),
        pltpu.make_async_copy(prompt.at[1], pbuf.at[1], lsem.at[1]),
        pltpu.make_async_copy(kw, wbuf.at[0, 0], lsem.at[2]),
        pltpu.make_async_copy(vw, wbuf.at[0, 1], lsem.at[3]),
    ]
    for load in loads:
        load.start()

    barrier = pltpu.get_barrier_semaphore()
    for dy, dx in ORDER[1:]:
        pl.semaphore_signal(barrier, inc=1, device_id=(sp, plane(dy, dx)), device_id_type=MESH)
    for step in range(1, 2 * Z):
        pl.semaphore_signal(barrier, inc=1, device_id=(lax.rem(sp + step, 2 * Z), tp), device_id_type=MESH)

    gain_row = gain[...]

    def norm(parity):
        loads[parity].wait()

        @pl.loop(0, POS // 32)
        def _(step):
            rows = pl.ds(pl.multiple_of(step * 32, 32), 32)
            flat = pbuf[parity, rows, :].astype(jnp.float32)
            scale = lax.rsqrt(jnp.mean(flat * flat, axis=-1, keepdims=True) + EPS)
            nbuf[parity, rows, :] = (flat * scale * gain_row).astype(jnp.bfloat16)

    norm(0)
    loads[2].wait()
    loads[3].wait()
    pl.semaphore_wait(barrier, 15 + 2 * Z - 1)

    sends = []

    def unit(j):
        return nbuf.at[0, pl.ds(pl.multiple_of(j * UNIT, UNIT), UNIT), :]

    own = pltpu.make_async_copy(unit(tp), ubuf.at[tp], ur.at[tp])
    own.start()
    for slot, (dy, dx) in enumerate(ORDER[1:]):
        j = plane(dy, dx)
        copy = remote(unit(j), ubuf.at[tp], us.at[slot], ur.at[tp], (sp, j))
        copy.start()
        sends.append(copy)

    for i, offset in enumerate(ORDER[1:7]):
        copy = remote(wbuf.at[0, c], wbuf.at[SLOT[offset], c], ws.at[i], wr.at[SLOT[offset]],
                      (sp, plane(-offset[0], -offset[1])))
        copy.start()
        sends.append(copy)

    norm(1)

    rows_here = xbuf.at[pl.ds(pl.multiple_of(z * UNIT, UNIT), UNIT), :]
    local_unit = None
    for i, d in enumerate(STEPS):
        t = lax.rem(z + d + Z, Z)
        pltpu.make_async_copy(ubuf.at[t], ubuf.at[t], ur.at[t]).wait()
        if d == 0:
            local_unit = pltpu.make_async_copy(ubuf.at[t], rows_here, bs.at[i])
            local_unit.start()
        else:
            copy = remote(ubuf.at[t], rows_here, bs.at[i], br.at[z], (t * 2 + c, tp))
            copy.start()
            sends.append(copy)

    eye = lax.broadcasted_iota(jnp.int32, (HEAD, HEAD), 0) == lax.broadcasted_iota(jnp.int32, (HEAD, HEAD), 1)
    gain_col = jnp.sum(jnp.where(eye, kgain[...], 0.0), axis=1, keepdims=True)

    def project(lo, hi):
        count = hi - lo
        weights = wbuf[lo:hi].reshape(count * 2 * HEAD, D)
        raw = lax.dot_general(weights, nbuf[1], (((1,), (1,)), ((), ())), preferred_element_type=jnp.float32)
        for i in range(count):
            key = raw[i * 2 * HEAD: i * 2 * HEAD + HEAD]
            scale = lax.rsqrt(jnp.mean(key * key, axis=0, keepdims=True) + EPS)
            sbuf[lo + i, 0] = (key * scale * gain_col).astype(jnp.bfloat16)
            sbuf[lo + i, 1] = raw[i * 2 * HEAD + HEAD: (i + 1) * 2 * HEAD].astype(jnp.bfloat16)

    def arrive(slot):
        half = remote(wbuf.at[slot, c], wbuf.at[slot, c], ps.at[slot], wr.at[slot], partner)
        half.wait_recv()
        over = remote(wbuf.at[slot, c], wbuf.at[slot, c], ps.at[slot], pr.at[slot], partner)
        over.start()
        sends.append(over)

    def other(slot):
        remote(wbuf.at[slot, 1 - c], wbuf.at[slot, 1 - c], ps.at[slot], pr.at[slot], partner).wait_recv()

    def spread(step):
        source = jnp.where(first, SLOT[(step, 0)], SLOT[(0, step)])
        for hop in (1, 3, 2):
            slot = jnp.where(first, SLOT[(step, hop)], SLOT[(hop, step)])
            target = jnp.where(first, plane(0, -hop), plane(-hop, 0))
            copy = remote(wbuf.at[source, c], wbuf.at[slot, c], fs.at[step * 4 + hop], wr.at[slot], (sp, target))
            copy.start()
            sends.append(copy)

    def hand(slot):
        dy, dx = ORDER[slot]
        if slot == 0:
            pltpu.make_async_copy(sbuf.at[slot], mbuf.at[tp], mr.at[tp]).start()
        else:
            copy = remote(sbuf.at[slot], mbuf.at[tp], ms.at[slot], mr.at[tp], (sp, plane(dy, dx)))
            copy.start()
            sends.append(copy)

    project(0, 1)
    hand(0)
    for number, (lo, hi) in enumerate(GROUPS):
        for slot in range(lo, hi):
            arrive(slot)
        if number == 0:
            spread(1)
            spread(3)
        if number == 1:
            spread(2)
        for slot in range(lo, hi):
            other(slot)
        project(lo, hi)
        for slot in range(lo, hi):
            hand(slot)

    columns = kv.at[:, :, pl.ds(pl.multiple_of(sp * POS, POS), POS)]
    for i, d in enumerate(STEPS):
        t = lax.rem(z + d + Z, Z)
        pltpu.make_async_copy(mbuf.at[t], mbuf.at[t], mr.at[t]).wait()
        far = remote(mbuf.at[t], columns, zs.at[i], zr.at[sp], (t * 2 + 1, tp))
        if d == 0:
            near = pltpu.make_async_copy(mbuf.at[t], columns, zs.at[i])

            @pl.when(first)
            def _():
                far.start()

            @pl.when(jnp.logical_not(first))
            def _():
                near.start()
        else:
            far.start()
            sends.append(far)

    local_unit.wait()
    for d in STEPS:
        if d != 0:
            s = lax.rem(z + d + Z, Z)
            came = xbuf.at[pl.ds(pl.multiple_of(s * UNIT, UNIT), UNIT), :]
            remote(came, came, bs.at[0], br.at[s], partner).wait_recv()

    lane = lax.broadcasted_iota(jnp.int32, (1, 2 * HEAD), 1)
    gain_both = jnp.concatenate([kgain[...], kgain[...]], axis=1)
    place = tbuf.at[:, c, tp]
    for slot, (dy, dx) in enumerate(ORDER):
        weights = wbuf[slot].reshape(2 * HEAD, D)
        raw = lax.dot_general(xbuf[...], weights, (((1,), (1,)), ((), ())), preferred_element_type=jnp.float32)
        mean = jnp.sum(jnp.where(lane < HEAD, raw * raw, 0.0), axis=1, keepdims=True) * (1.0 / HEAD)
        scale = jnp.where(lane < HEAD, lax.rsqrt(mean + EPS) * gain_both, 1.0)
        ybuf[slot] = (raw * scale).astype(jnp.bfloat16).reshape(Z, UNIT, 2 * HEAD)
        far = remote(ybuf.at[slot], place, ys.at[slot], yr.at[tp * 2 + c], (z * 2, plane(dy, dx)))
        if slot == 0:
            near_y = pltpu.make_async_copy(ybuf.at[slot], place, ys.at[slot])
            far_y = far

            @pl.when(first)
            def _():
                near_y.start()

            @pl.when(jnp.logical_not(first))
            def _():
                far_y.start()
        else:
            far.start()
            sends.append(far)

    @pl.when(first)
    def _():
        near_y.wait()

        @pl.loop(0, 2 * 16)
        def _(source):
            @pl.when(source != tp * 2)
            def _():
                came = tbuf.at[:, lax.rem(source, 2), source // 2]
                remote(came, came, ys.at[0], yr.at[source], partner).wait_recv()

        one = lax.broadcasted_iota(jnp.int32, (128, 128), 0) == lax.broadcasted_iota(jnp.int32, (128, 128), 1)
        identity = jnp.where(one, 1.0, 0.0).astype(jnp.bfloat16)

        @pl.loop(0, 2 * Z)
        def _(p):
            rows = tbuf[p // 2, lax.rem(p, 2)].reshape(POS, 2 * HEAD)
            turned = lax.dot_general(identity, rows, (((1,), (1,)), ((), ())), preferred_element_type=jnp.float32)
            turned = turned.astype(jnp.bfloat16)
            span = pl.ds(pl.multiple_of(p * POS, POS), POS)
            kvbuf[0, :, span] = turned[:HEAD]
            kvbuf[1, :, span] = turned[HEAD:]

        out = pltpu.make_async_copy(kvbuf, kv, lsem.at[0])
        out.start()
        out.wait()
        far_d0 = remote(mbuf.at[z], columns, zs.at[STEPS.index(0)], zr.at[sp], (z * 2 + 1, tp))
        far_d0.wait_send()

    @pl.when(jnp.logical_not(first))
    def _():
        far_y.wait_send()
        pltpu.make_async_copy(mbuf.at[z], columns, zs.at[STEPS.index(0)]).wait()

        @pl.loop(0, 2 * Z)
        def _(p):
            @pl.when(p != sp)
            def _():
                span = kv.at[:, :, pl.ds(pl.multiple_of(p * POS, POS), POS)]
                remote(span, span, zs.at[0], zr.at[p], partner).wait_recv()

    for copy in sends:
        copy.wait_send()


def read(kv, queries, bias, keys, values, out, kbuf, vbuf, lsem, ssem):
    length = kbuf.shape[1]
    head = lax.axis_index("tp")
    load_k = pltpu.make_async_copy(kv.at[0], kbuf, lsem.at[0])
    load_v = pltpu.make_async_copy(kv.at[1], vbuf, lsem.at[1])
    load_k.start()
    load_v.start()
    load_k.wait()
    store_k = pltpu.make_async_copy(kbuf, keys.at[0], ssem.at[0])
    store_k.start()
    q = jnp.concatenate([queries[0], jnp.zeros((6, HEAD), jnp.bfloat16)], axis=0)
    scores = jnp.dot(q, kbuf[...], preferred_element_type=jnp.float32) * 0.125
    row = lax.broadcasted_iota(jnp.int32, (8, 1), 0)
    scores = scores + jnp.where(row == 0, bias[0, head], bias[1, head])
    soft = jnp.log1p(jnp.exp(-jnp.abs(scores)))
    log_break = jnp.minimum(scores, 0.0) - soft
    log_keep = jnp.minimum(-scores, 0.0) - soft
    blocks = length // 128
    stacked = jnp.concatenate([log_keep[:, b * 128:(b + 1) * 128] for b in range(blocks)], axis=0)
    r = lax.broadcasted_iota(jnp.int32, (128, 256), 0)
    col = lax.broadcasted_iota(jnp.int32, (128, 256), 1)
    tri = jnp.where((r > col) | (col >= 128), 1.0, 0.0).astype(jnp.float32)
    sums = jnp.dot(stacked, tri, preferred_element_type=jnp.float32, precision=lax.Precision.HIGHEST)
    carry = jnp.zeros((8, 128), jnp.float32)
    parts = [None] * blocks
    for b in range(blocks - 1, -1, -1):
        parts[b] = sums[b * 8:(b + 1) * 8, :128] + carry
        carry = carry + sums[b * 8:(b + 1) * 8, 128:]
    later = jnp.concatenate(parts, axis=1)
    weights = jnp.exp(log_break + later).astype(jnp.bfloat16)
    load_v.wait()
    store_v = pltpu.make_async_copy(vbuf, values.at[0], ssem.at[1])
    store_v.start()
    result = lax.dot_general(weights, vbuf[...], (((1,), (1,)), ((), ())), preferred_element_type=jnp.float32)
    out[0] = result[:2].astype(jnp.bfloat16)
    store_k.wait()
    store_v.wait()


def local(prompt, input_gain, key_weight, value_weight, key_gain, queries, score_bias):
    hbm = pl.BlockSpec(memory_space=pltpu.HBM)
    vmem = pl.BlockSpec(memory_space=pltpu.VMEM)
    length = POS * 2 * Z
    dma = pltpu.SemaphoreType.DMA
    bf16 = jnp.bfloat16
    kv = pl.pallas_call(
        exchange,
        out_shape=jax.ShapeDtypeStruct((2, HEAD, length), jnp.bfloat16),
        in_specs=[hbm, vmem, hbm, hbm, vmem],
        out_specs=hbm,
        scratch_shapes=[
            pltpu.VMEM((2, POS, D), bf16),
            pltpu.VMEM((2, POS, D), bf16),
            pltpu.VMEM((16, UNIT, D), bf16),
            pltpu.VMEM((Z * UNIT, D), bf16),
            pltpu.VMEM((16, 2, HEAD, D), bf16),
            pltpu.VMEM((16, 2, HEAD, POS), bf16),
            pltpu.VMEM((16, 2, HEAD, POS), bf16),
            pltpu.VMEM((16, Z, UNIT, 2 * HEAD), bf16),
            pltpu.VMEM((Z, 2, 16, UNIT, 2 * HEAD), bf16),
            pltpu.VMEM((2, HEAD, length), bf16),
            dma((4,)), dma((15,)), dma((16,)), dma((16,)), dma((16,)), dma((6,)), dma((16,)), dma((16,)),
            dma((16,)), dma((16,)), dma((16,)), dma((16,)), dma((16,)), dma((32,)), dma((16,)), dma((32,)),
        ],
        compiler_params=pltpu.CompilerParams(collective_id=0, has_side_effects=True),
        name="exchange",
    )(prompt, input_gain.reshape(1, D), key_weight, value_weight, key_gain.reshape(1, HEAD))
    keys, values, out = pl.pallas_call(
        read,
        out_shape=(
            jax.ShapeDtypeStruct((1, HEAD, length), jnp.bfloat16),
            jax.ShapeDtypeStruct((1, HEAD, length), jnp.bfloat16),
            jax.ShapeDtypeStruct((1, 2, HEAD), jnp.bfloat16),
        ),
        in_specs=[hbm, vmem, pl.BlockSpec(memory_space=pltpu.SMEM)],
        out_specs=(hbm, hbm, vmem),
        scratch_shapes=[
            pltpu.VMEM((HEAD, length), jnp.bfloat16),
            pltpu.VMEM((HEAD, length), jnp.bfloat16),
            dma((2,)), dma((2,)),
        ],
        name="read",
    )(kv, queries, score_bias)
    return keys, values, out


def solution(mesh):
    placed = (P("tp", "sp", None), P(), P("tp", None), P("tp", None), P(), P("sp", None, "tp"), P())
    return jax.shard_map(
        local,
        mesh=mesh,
        in_specs=placed,
        out_specs=(P("sp", "tp", None), P("sp", "tp", None), P("sp", None, "tp")),
        check_vma=False,
    )
```

```python
import jax
import jax.numpy as jnp
from jax import lax
from jax.experimental import pallas as pl
from jax.experimental.pallas import tpu as pltpu
from jax.sharding import PartitionSpec as P

HEAD = 64
EPS = 1e-06
MESH = pl.DeviceIdType.MESH
Y, X, Z = 4, 4, 16
POS = 256
D = 2048

ORDER = [(0, 0), (1, 0), (3, 0), (0, 1), (0, 3), (2, 0), (0, 2),
         (1, 1), (1, 3), (3, 1), (3, 3), (2, 1), (2, 3), (1, 2), (3, 2), (2, 2)]
SLOT = {offset: slot for slot, offset in enumerate(ORDER)}
UNIT = 16
STEPS = [8, 7, -7, 6, -6, 5, -5, 4, -4, 3, -3, 2, -2, 1, -1, 0]
GROUPS = [(1, 5), (5, 7), (7, 11), (11, 15), (15, 16)]


def exchange(prompt, gain, kw, vw, kgain, kv, pbuf, nbuf, ubuf, xbuf, wbuf, sbuf, mbuf, ybuf, tbuf, kvbuf,
             tok, lsem, us, ur, bs, br, ws, wr, fs, ps, pr, ms, mr, zs, zr, ys, yr):
    sp = lax.axis_index("sp")
    tp = lax.axis_index("tp")
    z, c = sp // 2, lax.rem(sp, 2)
    y, x = tp // X, lax.rem(tp, X)
    first = c == 0
    partner = (z * 2 + 1 - c, tp)

    def plane(dy, dx):
        return lax.rem(y + dy + Y, Y) * X + lax.rem(x + dx + X, X)

    def remote(src, dst, send, recv, device):
        return pltpu.make_async_remote_copy(src_ref=src, dst_ref=dst, send_sem=send, recv_sem=recv,
                                            device_id=device, device_id_type=MESH)

    loads = [
        pltpu.make_async_copy(prompt.at[1], pbuf, lsem.at[0]),
        pltpu.make_async_copy(kw, wbuf.at[0, 0], lsem.at[1]),
        pltpu.make_async_copy(vw, wbuf.at[0, 1], lsem.at[2]),
    ]
    for load in loads:
        load.start()

    barrier = pltpu.get_barrier_semaphore()
    for dy, dx in ORDER[1:]:
        pl.semaphore_signal(barrier, inc=1, device_id=(sp, plane(dy, dx)), device_id_type=MESH)
    ahead = (lax.rem(sp + 2, 2 * Z), tp)
    behind = (lax.rem(sp + 2 * Z - 2, 2 * Z), tp)
    for device in (partner, ahead, behind):
        pl.semaphore_signal(barrier, inc=1, device_id=device, device_id_type=MESH)

    gain_row = gain[...]

    def norm(source, target):
        @pl.loop(0, POS // 32)
        def _(step):
            rows = pl.ds(pl.multiple_of(step * 32, 32), 32)
            flat = source[rows, :].astype(jnp.float32)
            scale = lax.rsqrt(jnp.mean(flat * flat, axis=-1, keepdims=True) + EPS)
            target[rows, :] = (flat * scale * gain_row).astype(jnp.bfloat16)

    pl.semaphore_wait(barrier, 15 + 3)

    sends = []

    def unit(j):
        return prompt.at[0, pl.ds(pl.multiple_of(j * UNIT, UNIT), UNIT), :]

    own = pltpu.make_async_copy(unit(tp), ubuf.at[tp], ur.at[tp])
    own.start()
    for slot, (dy, dx) in enumerate(ORDER[1:]):
        j = plane(dy, dx)
        copy = remote(unit(j), ubuf.at[tp], us.at[slot], ur.at[tp], (sp, j))
        copy.start()
        sends.append(copy)

    loads[1].wait()
    loads[2].wait()
    for i, offset in enumerate(ORDER[1:7]):
        copy = remote(wbuf.at[0, c], wbuf.at[SLOT[offset], c], ws.at[i], wr.at[SLOT[offset]],
                      (sp, plane(-offset[0], -offset[1])))
        copy.start()
        sends.append(copy)

    rows_here = xbuf.at[pl.ds(pl.multiple_of(z * UNIT, UNIT), UNIT), :]
    local_unit = None
    for i, hop in enumerate((1, 2, 4)):
        for side, d in enumerate((hop, -hop)):
            pl.semaphore_signal(tok.at[i, side], inc=1, device_id=(lax.rem(sp + 2 * d + 2 * Z, 2 * Z), tp),
                                device_id_type=MESH)
        for side in range(2):
            pl.semaphore_wait(tok.at[i, side], 1)
    for i, d in enumerate(STEPS):
        t = lax.rem(z + d + Z, Z)
        pltpu.make_async_copy(ubuf.at[t], ubuf.at[t], ur.at[t]).wait()
        if d == 0:
            local_unit = pltpu.make_async_copy(ubuf.at[t], rows_here, bs.at[i])
            local_unit.start()
        else:
            copy = remote(ubuf.at[t], rows_here, bs.at[i], br.at[z], (t * 2 + c, tp))
            copy.start()
            sends.append(copy)

    loads[0].wait()
    norm(pbuf, nbuf)

    eye = lax.broadcasted_iota(jnp.int32, (HEAD, HEAD), 0) == lax.broadcasted_iota(jnp.int32, (HEAD, HEAD), 1)
    gain_col = jnp.sum(jnp.where(eye, kgain[...], 0.0), axis=1, keepdims=True)

    def project(lo, hi):
        count = hi - lo
        weights = wbuf[lo:hi].reshape(count * 2 * HEAD, D)
        raw = lax.dot_general(weights, nbuf[...], (((1,), (1,)), ((), ())), preferred_element_type=jnp.float32)
        for i in range(count):
            key = raw[i * 2 * HEAD: i * 2 * HEAD + HEAD]
            scale = lax.rsqrt(jnp.mean(key * key, axis=0, keepdims=True) + EPS)
            sbuf[lo + i, 0] = (key * scale * gain_col).astype(jnp.bfloat16)
            sbuf[lo + i, 1] = raw[i * 2 * HEAD + HEAD: (i + 1) * 2 * HEAD].astype(jnp.bfloat16)

    def arrive(slot):
        half = remote(wbuf.at[slot, c], wbuf.at[slot, c], ps.at[slot], wr.at[slot], partner)
        half.wait_recv()
        over = remote(wbuf.at[slot, c], wbuf.at[slot, c], ps.at[slot], pr.at[slot], partner)
        over.start()
        sends.append(over)

    def other(slot):
        remote(wbuf.at[slot, 1 - c], wbuf.at[slot, 1 - c], ps.at[slot], pr.at[slot], partner).wait_recv()

    def spread(step):
        source = jnp.where(first, SLOT[(step, 0)], SLOT[(0, step)])
        for hop in (1, 3, 2):
            slot = jnp.where(first, SLOT[(step, hop)], SLOT[(hop, step)])
            target = jnp.where(first, plane(0, -hop), plane(-hop, 0))
            copy = remote(wbuf.at[source, c], wbuf.at[slot, c], fs.at[step * 4 + hop], wr.at[slot], (sp, target))
            copy.start()
            sends.append(copy)

    def hand(slot):
        dy, dx = ORDER[slot]
        if slot == 0:
            pltpu.make_async_copy(sbuf.at[slot], mbuf.at[tp], mr.at[tp]).start()
        else:
            copy = remote(sbuf.at[slot], mbuf.at[tp], ms.at[slot], mr.at[tp], (sp, plane(dy, dx)))
            copy.start()
            sends.append(copy)

    project(0, 1)
    hand(0)
    for number, (lo, hi) in enumerate(GROUPS):
        for slot in range(lo, hi):
            arrive(slot)
        if number == 0:
            spread(1)
            spread(3)
        if number == 1:
            spread(2)
        for slot in range(lo, hi):
            other(slot)
        project(lo, hi)
        for slot in range(lo, hi):
            hand(slot)

    columns = kv.at[:, :, pl.ds(pl.multiple_of(sp * POS, POS), POS)]
    for i, d in enumerate(STEPS):
        t = lax.rem(z + d + Z, Z)
        pltpu.make_async_copy(mbuf.at[t], mbuf.at[t], mr.at[t]).wait()
        far = remote(mbuf.at[t], columns, zs.at[i], zr.at[sp], (t * 2 + 1, tp))
        if d == 0:
            near = pltpu.make_async_copy(mbuf.at[t], columns, zs.at[i])

            @pl.when(first)
            def _():
                far.start()

            @pl.when(jnp.logical_not(first))
            def _():
                near.start()
        else:
            far.start()
            sends.append(far)

    local_unit.wait()
    for d in STEPS:
        if d != 0:
            s = lax.rem(z + d + Z, Z)
            came = xbuf.at[pl.ds(pl.multiple_of(s * UNIT, UNIT), UNIT), :]
            remote(came, came, bs.at[0], br.at[s], partner).wait_recv()

    norm(xbuf, xbuf)
    lane = lax.broadcasted_iota(jnp.int32, (1, 2 * HEAD), 1)
    gain_both = jnp.concatenate([kgain[...], kgain[...]], axis=1)
    place = tbuf.at[:, c, tp]
    for slot, (dy, dx) in enumerate(ORDER):
        weights = wbuf[slot].reshape(2 * HEAD, D)
        raw = lax.dot_general(xbuf[...], weights, (((1,), (1,)), ((), ())), preferred_element_type=jnp.float32)
        mean = jnp.sum(jnp.where(lane < HEAD, raw * raw, 0.0), axis=1, keepdims=True) * (1.0 / HEAD)
        scale = jnp.where(lane < HEAD, lax.rsqrt(mean + EPS) * gain_both, 1.0)
        ybuf[slot] = (raw * scale).astype(jnp.bfloat16).reshape(Z, UNIT, 2 * HEAD)
        far = remote(ybuf.at[slot], place, ys.at[slot], yr.at[tp * 2 + c], (z * 2, plane(dy, dx)))
        if slot == 0:
            near_y = pltpu.make_async_copy(ybuf.at[slot], place, ys.at[slot])
            far_y = far

            @pl.when(first)
            def _():
                near_y.start()

            @pl.when(jnp.logical_not(first))
            def _():
                far_y.start()
        else:
            far.start()
            sends.append(far)

    @pl.when(first)
    def _():
        near_y.wait()

        @pl.loop(0, 2 * 16)
        def _(source):
            @pl.when(source != tp * 2)
            def _():
                came = tbuf.at[:, lax.rem(source, 2), source // 2]
                remote(came, came, ys.at[0], yr.at[source], partner).wait_recv()

        one = lax.broadcasted_iota(jnp.int32, (128, 128), 0) == lax.broadcasted_iota(jnp.int32, (128, 128), 1)
        identity = jnp.where(one, 1.0, 0.0).astype(jnp.bfloat16)

        @pl.loop(0, 2 * Z)
        def _(p):
            rows = tbuf[p // 2, lax.rem(p, 2)].reshape(POS, 2 * HEAD)
            turned = lax.dot_general(identity, rows, (((1,), (1,)), ((), ())), preferred_element_type=jnp.float32)
            turned = turned.astype(jnp.bfloat16)
            span = pl.ds(pl.multiple_of(p * POS, POS), POS)
            kvbuf[0, :, span] = turned[:HEAD]
            kvbuf[1, :, span] = turned[HEAD:]

        out = pltpu.make_async_copy(kvbuf, kv, lsem.at[0])
        out.start()
        out.wait()
        far_d0 = remote(mbuf.at[z], columns, zs.at[STEPS.index(0)], zr.at[sp], (z * 2 + 1, tp))
        far_d0.wait_send()

    @pl.when(jnp.logical_not(first))
    def _():
        far_y.wait_send()
        pltpu.make_async_copy(mbuf.at[z], columns, zs.at[STEPS.index(0)]).wait()

        @pl.loop(0, 2 * Z)
        def _(p):
            @pl.when(p != sp)
            def _():
                span = kv.at[:, :, pl.ds(pl.multiple_of(p * POS, POS), POS)]
                remote(span, span, zs.at[0], zr.at[p], partner).wait_recv()

    for copy in sends:
        copy.wait_send()


def read(kv, queries, bias, keys, values, out, kbuf, vbuf, lsem, ssem):
    length = kbuf.shape[1]
    head = lax.axis_index("tp")
    load_k = pltpu.make_async_copy(kv.at[0], kbuf, lsem.at[0])
    load_v = pltpu.make_async_copy(kv.at[1], vbuf, lsem.at[1])
    load_k.start()
    load_v.start()
    load_k.wait()
    store_k = pltpu.make_async_copy(kbuf, keys.at[0], ssem.at[0])
    store_k.start()
    q = jnp.concatenate([queries[0], jnp.zeros((6, HEAD), jnp.bfloat16)], axis=0)
    scores = jnp.dot(q, kbuf[...], preferred_element_type=jnp.float32) * 0.125
    row = lax.broadcasted_iota(jnp.int32, (8, 1), 0)
    scores = scores + jnp.where(row == 0, bias[0, head], bias[1, head])
    soft = jnp.log1p(jnp.exp(-jnp.abs(scores)))
    log_break = jnp.minimum(scores, 0.0) - soft
    log_keep = jnp.minimum(-scores, 0.0) - soft
    blocks = length // 128
    stacked = jnp.concatenate([log_keep[:, b * 128:(b + 1) * 128] for b in range(blocks)], axis=0)
    r = lax.broadcasted_iota(jnp.int32, (128, 256), 0)
    col = lax.broadcasted_iota(jnp.int32, (128, 256), 1)
    tri = jnp.where((r > col) | (col >= 128), 1.0, 0.0).astype(jnp.float32)
    sums = jnp.dot(stacked, tri, preferred_element_type=jnp.float32, precision=lax.Precision.HIGHEST)
    carry = jnp.zeros((8, 128), jnp.float32)
    parts = [None] * blocks
    for b in range(blocks - 1, -1, -1):
        parts[b] = sums[b * 8:(b + 1) * 8, :128] + carry
        carry = carry + sums[b * 8:(b + 1) * 8, 128:]
    later = jnp.concatenate(parts, axis=1)
    weights = jnp.exp(log_break + later).astype(jnp.bfloat16)
    load_v.wait()
    store_v = pltpu.make_async_copy(vbuf, values.at[0], ssem.at[1])
    store_v.start()
    result = lax.dot_general(weights, vbuf[...], (((1,), (1,)), ((), ())), preferred_element_type=jnp.float32)
    out[0] = result[:2].astype(jnp.bfloat16)
    store_k.wait()
    store_v.wait()


def local(prompt, input_gain, key_weight, value_weight, key_gain, queries, score_bias):
    hbm = pl.BlockSpec(memory_space=pltpu.HBM)
    vmem = pl.BlockSpec(memory_space=pltpu.VMEM)
    length = POS * 2 * Z
    dma = pltpu.SemaphoreType.DMA
    bf16 = jnp.bfloat16
    kv = pl.pallas_call(
        exchange,
        out_shape=jax.ShapeDtypeStruct((2, HEAD, length), jnp.bfloat16),
        in_specs=[hbm, vmem, hbm, hbm, vmem],
        out_specs=hbm,
        scratch_shapes=[
            pltpu.VMEM((POS, D), bf16),
            pltpu.VMEM((POS, D), bf16),
            pltpu.VMEM((16, UNIT, D), bf16),
            pltpu.VMEM((Z * UNIT, D), bf16),
            pltpu.VMEM((16, 2, HEAD, D), bf16),
            pltpu.VMEM((16, 2, HEAD, POS), bf16),
            pltpu.VMEM((16, 2, HEAD, POS), bf16),
            pltpu.VMEM((16, Z, UNIT, 2 * HEAD), bf16),
            pltpu.VMEM((Z, 2, 16, UNIT, 2 * HEAD), bf16),
            pltpu.VMEM((2, HEAD, length), bf16),
            pltpu.SemaphoreType.REGULAR((8, 2)), dma((3,)), dma((15,)), dma((16,)), dma((16,)), dma((16,)), dma((6,)), dma((16,)), dma((16,)),
            dma((16,)), dma((16,)), dma((16,)), dma((16,)), dma((16,)), dma((32,)), dma((16,)), dma((32,)),
        ],
        compiler_params=pltpu.CompilerParams(collective_id=0, has_side_effects=True),
        name="exchange",
    )(prompt, input_gain.reshape(1, D), key_weight, value_weight, key_gain.reshape(1, HEAD))
    keys, values, out = pl.pallas_call(
        read,
        out_shape=(
            jax.ShapeDtypeStruct((1, HEAD, length), jnp.bfloat16),
            jax.ShapeDtypeStruct((1, HEAD, length), jnp.bfloat16),
            jax.ShapeDtypeStruct((1, 2, HEAD), jnp.bfloat16),
        ),
        in_specs=[hbm, vmem, pl.BlockSpec(memory_space=pltpu.SMEM)],
        out_specs=(hbm, hbm, vmem),
        scratch_shapes=[
            pltpu.VMEM((HEAD, length), jnp.bfloat16),
            pltpu.VMEM((HEAD, length), jnp.bfloat16),
            dma((2,)), dma((2,)),
        ],
        name="read",
    )(kv, queries, score_bias)
    return keys, values, out


def solution(mesh):
    placed = (P("tp", "sp", None), P(), P("tp", None), P("tp", None), P(), P("sp", None, "tp"), P())
    return jax.shard_map(
        local,
        mesh=mesh,
        in_specs=placed,
        out_specs=(P("sp", "tp", None), P("sp", "tp", None), P("sp", None, "tp")),
        check_vma=False,
    )
```

```python
import jax
import jax.numpy as jnp
from jax import lax
from jax.experimental import pallas as pl
from jax.experimental.pallas import tpu as pltpu
from jax.sharding import PartitionSpec as P

HEAD = 64
EPS = 1e-06
MESH = pl.DeviceIdType.MESH
Y, X, Z = 4, 4, 16
POS = 256
D = 2048

ORDER = [(0, 0), (1, 0), (3, 0), (0, 1), (0, 3), (2, 0), (0, 2),
         (1, 1), (1, 3), (3, 1), (3, 3), (2, 1), (2, 3), (1, 2), (3, 2), (2, 2)]
SLOT = {offset: slot for slot, offset in enumerate(ORDER)}
UNIT = 16
STEPS = [8, 7, -7, 6, -6, 5, -5, 4, -4, 3, -3, 2, -2, 1, -1, 0]
LATER = [0, 8, 7, -7, 6, -6, 5, -5, 4, -4, 3, -3, 2, -2, 1, -1]
GROUPS = [(1, 5), (5, 7), (7, 11), (11, 15), (15, 16)]


def exchange(prompt, gain, kw, vw, kgain, queries, bias, kv, result, pbuf, nbuf, ubuf, xbuf, wbuf, sbuf, mbuf, ybuf, tbuf, parts, totals,
             tok, lsem, us, ur, bs, br, ws, wr, fs, ps, pr, ms, mr, zs, zr, ys, yr):
    sp = lax.axis_index("sp")
    tp = lax.axis_index("tp")
    z, c = sp // 2, lax.rem(sp, 2)
    y, x = tp // X, lax.rem(tp, X)
    first = c == 0
    partner = (z * 2 + 1 - c, tp)

    def plane(dy, dx):
        return lax.rem(y + dy + Y, Y) * X + lax.rem(x + dx + X, X)

    def remote(src, dst, send, recv, device):
        return pltpu.make_async_remote_copy(src_ref=src, dst_ref=dst, send_sem=send, recv_sem=recv,
                                            device_id=device, device_id_type=MESH)

    loads = [
        pltpu.make_async_copy(prompt.at[1], pbuf, lsem.at[0]),
        pltpu.make_async_copy(kw, wbuf.at[0, 0], lsem.at[1]),
        pltpu.make_async_copy(vw, wbuf.at[0, 1], lsem.at[2]),
    ]
    for load in loads:
        load.start()

    barrier = pltpu.get_barrier_semaphore()
    for dy, dx in ORDER[1:]:
        pl.semaphore_signal(barrier, inc=1, device_id=(sp, plane(dy, dx)), device_id_type=MESH)
    ahead = (lax.rem(sp + 2, 2 * Z), tp)
    behind = (lax.rem(sp + 2 * Z - 2, 2 * Z), tp)
    for device in (partner, ahead, behind):
        pl.semaphore_signal(barrier, inc=1, device_id=device, device_id_type=MESH)

    gain_row = gain[...]

    def norm(source, target):
        @pl.loop(0, POS // 32)
        def _(step):
            rows = pl.ds(pl.multiple_of(step * 32, 32), 32)
            flat = source[rows, :].astype(jnp.float32)
            scale = lax.rsqrt(jnp.mean(flat * flat, axis=-1, keepdims=True) + EPS)
            target[rows, :] = (flat * scale * gain_row).astype(jnp.bfloat16)

    pl.semaphore_wait(barrier, 15 + 3)

    sends = []

    def unit(j):
        return prompt.at[0, pl.ds(pl.multiple_of(j * UNIT, UNIT), UNIT), :]

    own = pltpu.make_async_copy(unit(tp), ubuf.at[tp], ur.at[tp])
    own.start()
    for slot, (dy, dx) in enumerate(ORDER[1:]):
        j = plane(dy, dx)
        copy = remote(unit(j), ubuf.at[tp], us.at[slot], ur.at[tp], (sp, j))
        copy.start()
        sends.append(copy)

    loads[1].wait()
    loads[2].wait()
    for i, offset in enumerate(ORDER[1:7]):
        copy = remote(wbuf.at[0, c], wbuf.at[SLOT[offset], c], ws.at[i], wr.at[SLOT[offset]],
                      (sp, plane(-offset[0], -offset[1])))
        copy.start()
        sends.append(copy)

    rows_here = xbuf.at[pl.ds(pl.multiple_of(z * UNIT, UNIT), UNIT), :]
    local_unit = None
    for i, hop in enumerate((1, 2, 4)):
        for side, d in enumerate((hop, -hop)):
            pl.semaphore_signal(tok.at[i, side], inc=1, device_id=(lax.rem(sp + 2 * d + 2 * Z, 2 * Z), tp),
                                device_id_type=MESH)
        for side in range(2):
            pl.semaphore_wait(tok.at[i, side], 1)
    for i, d in enumerate(STEPS):
        t = lax.rem(z + d + Z, Z)
        pltpu.make_async_copy(ubuf.at[t], ubuf.at[t], ur.at[t]).wait()
        if d == 0:
            local_unit = pltpu.make_async_copy(ubuf.at[t], rows_here, bs.at[i])
            local_unit.start()
        else:
            copy = remote(ubuf.at[t], rows_here, bs.at[i], br.at[z], (t * 2 + c, tp))
            copy.start()
            sends.append(copy)

    loads[0].wait()
    norm(pbuf, nbuf)

    eye = lax.broadcasted_iota(jnp.int32, (HEAD, HEAD), 0) == lax.broadcasted_iota(jnp.int32, (HEAD, HEAD), 1)
    gain_col = jnp.sum(jnp.where(eye, kgain[...], 0.0), axis=1, keepdims=True)

    def project(lo, hi):
        count = hi - lo
        weights = wbuf[lo:hi].reshape(count * 2 * HEAD, D)
        raw = lax.dot_general(weights, nbuf[...], (((1,), (1,)), ((), ())), preferred_element_type=jnp.float32)
        for i in range(count):
            key = raw[i * 2 * HEAD: i * 2 * HEAD + HEAD]
            scale = lax.rsqrt(jnp.mean(key * key, axis=0, keepdims=True) + EPS)
            sbuf[lo + i, 0] = (key * scale * gain_col).astype(jnp.bfloat16)
            sbuf[lo + i, 1] = raw[i * 2 * HEAD + HEAD: (i + 1) * 2 * HEAD].astype(jnp.bfloat16)

    def arrive(slot):
        half = remote(wbuf.at[slot, c], wbuf.at[slot, c], ps.at[slot], wr.at[slot], partner)
        half.wait_recv()
        over = remote(wbuf.at[slot, c], wbuf.at[slot, c], ps.at[slot], pr.at[slot], partner)
        over.start()
        sends.append(over)

    def other(slot):
        remote(wbuf.at[slot, 1 - c], wbuf.at[slot, 1 - c], ps.at[slot], pr.at[slot], partner).wait_recv()

    def spread(step):
        source = jnp.where(first, SLOT[(step, 0)], SLOT[(0, step)])
        for hop in (1, 3, 2):
            slot = jnp.where(first, SLOT[(step, hop)], SLOT[(hop, step)])
            target = jnp.where(first, plane(0, -hop), plane(-hop, 0))
            copy = remote(wbuf.at[source, c], wbuf.at[slot, c], fs.at[step * 4 + hop], wr.at[slot], (sp, target))
            copy.start()
            sends.append(copy)

    def hand(slot):
        dy, dx = ORDER[slot]
        if slot == 0:
            pltpu.make_async_copy(sbuf.at[slot], mbuf.at[tp], mr.at[tp]).start()
        else:
            copy = remote(sbuf.at[slot], mbuf.at[tp], ms.at[slot], mr.at[tp], (sp, plane(dy, dx)))
            copy.start()
            sends.append(copy)

    project(0, 1)
    hand(0)
    for number, (lo, hi) in enumerate(GROUPS):
        for slot in range(lo, hi):
            arrive(slot)
        if number == 0:
            spread(1)
            spread(3)
        if number == 1:
            spread(2)
        for slot in range(lo, hi):
            other(slot)
        project(lo, hi)
        for slot in range(lo, hi):
            hand(slot)

    columns = kv.at[:, :, pl.ds(pl.multiple_of(sp * POS, POS), POS)]
    for i, d in enumerate(LATER):
        t = lax.rem(z + d + Z, Z)
        pltpu.make_async_copy(mbuf.at[t], mbuf.at[t], mr.at[t]).wait()
        far = remote(mbuf.at[t], columns, zs.at[i], zr.at[sp], (t * 2 + 1, tp))
        if d == 0:
            near = pltpu.make_async_copy(mbuf.at[t], columns, zs.at[i])

            @pl.when(first)
            def _():
                far.start()

            @pl.when(jnp.logical_not(first))
            def _():
                near.start()
        else:
            far.start()
            sends.append(far)

    local_unit.wait()
    for d in STEPS:
        if d != 0:
            s = lax.rem(z + d + Z, Z)
            came = xbuf.at[pl.ds(pl.multiple_of(s * UNIT, UNIT), UNIT), :]
            remote(came, came, bs.at[0], br.at[s], partner).wait_recv()

    norm(xbuf, xbuf)
    lane = lax.broadcasted_iota(jnp.int32, (1, 2 * HEAD), 1)
    gain_both = jnp.concatenate([kgain[...], kgain[...]], axis=1)
    place = tbuf.at[:, c, tp]
    for slot, (dy, dx) in enumerate(ORDER):
        weights = wbuf[slot].reshape(2 * HEAD, D)
        raw = lax.dot_general(xbuf[...], weights, (((1,), (1,)), ((), ())), preferred_element_type=jnp.float32)
        mean = jnp.sum(jnp.where(lane < HEAD, raw * raw, 0.0), axis=1, keepdims=True) * (1.0 / HEAD)
        scale = jnp.where(lane < HEAD, lax.rsqrt(mean + EPS) * gain_both, 1.0)
        ybuf[slot] = (raw * scale).astype(jnp.bfloat16).reshape(Z, UNIT, 2 * HEAD)
        far = remote(ybuf.at[slot], place, ys.at[slot], yr.at[tp * 2 + c], (z * 2, plane(dy, dx)))
        if slot == 0:
            near_y = pltpu.make_async_copy(ybuf.at[slot], place, ys.at[slot])
            far_y = far

            @pl.when(first)
            def _():
                near_y.start()

            @pl.when(jnp.logical_not(first))
            def _():
                far_y.start()
        else:
            far.start()
            sends.append(far)

    @pl.when(first)
    def _():
        near_y.wait()

        @pl.loop(0, 2 * 16)
        def _(source):
            @pl.when(source != tp * 2)
            def _():
                came = tbuf.at[:, lax.rem(source, 2), source // 2]
                remote(came, came, ys.at[0], yr.at[source], partner).wait_recv()

        one = lax.broadcasted_iota(jnp.int32, (128, 128), 0) == lax.broadcasted_iota(jnp.int32, (128, 128), 1)
        identity = jnp.where(one, 1.0, 0.0).astype(jnp.bfloat16)

        @pl.loop(0, 2 * Z)
        def _(p):
            rows = tbuf[p // 2, lax.rem(p, 2)].reshape(POS, 2 * HEAD)
            turned = lax.dot_general(identity, rows, (((1,), (1,)), ((), ())), preferred_element_type=jnp.float32)
            turned = turned.astype(jnp.bfloat16)
            span = pl.ds(pl.multiple_of(p * POS, POS), POS)
            kv[0, :, span] = turned[:HEAD]
            kv[1, :, span] = turned[HEAD:]

    @pl.when(jnp.logical_not(first))
    def _():
        far_y.wait_send()
        pltpu.make_async_copy(mbuf.at[z], columns, zs.at[LATER.index(0)]).wait()

    q = jnp.concatenate([queries[0], jnp.zeros((6, HEAD), jnp.bfloat16)], axis=0)
    row = lax.broadcasted_iota(jnp.int32, (8, 1), 0)
    offset = jnp.where(row == 0, bias[0, tp], bias[1, tp])
    r = lax.broadcasted_iota(jnp.int32, (128, 256), 0)
    col = lax.broadcasted_iota(jnp.int32, (128, 256), 1)
    tri = jnp.where((r > col) | (col >= 128), 1.0, 0.0).astype(jnp.float32)
    span = 2 * POS

    @pl.loop(0, Z)
    def _(i):
        far_by = Z // 2 - i // 2
        d = jnp.where(i == 0, 0, jnp.where(lax.rem(i, 2) == 0, far_by, -far_by))
        s = lax.rem(z - d + Z, Z)

        @pl.when(jnp.logical_not(first))
        def _():
            for core in range(2):
                p = s * 2 + core

                @pl.when(p != sp)
                def _():
                    came = kv.at[:, :, pl.ds(pl.multiple_of(p * POS, POS), POS)]
                    remote(came, came, zs.at[0], zr.at[p], partner).wait_recv()

        at = pl.ds(pl.multiple_of(s * span, span), span)
        scores = jnp.dot(q, kv[0, :, at], preferred_element_type=jnp.float32) * 0.125 + offset
        soft = jnp.log1p(jnp.exp(-jnp.abs(scores)))
        log_break = jnp.minimum(scores, 0.0) - soft
        log_keep = jnp.minimum(-scores, 0.0) - soft
        stacked = jnp.concatenate([log_keep[:, b * 128:(b + 1) * 128] for b in range(span // 128)], axis=0)
        sums = jnp.dot(stacked, tri, preferred_element_type=jnp.float32, precision=lax.Precision.HIGHEST)
        carry = jnp.zeros((8, 128), jnp.float32)
        pieces = [None] * (span // 128)
        for b in range(span // 128 - 1, -1, -1):
            pieces[b] = sums[b * 8:(b + 1) * 8, :128] + carry
            carry = carry + sums[b * 8:(b + 1) * 8, 128:]
        weights = jnp.exp(log_break + jnp.concatenate(pieces, axis=1))
        high = weights.astype(jnp.bfloat16)
        low = (weights - high.astype(jnp.float32)).astype(jnp.bfloat16)
        both = lax.dot_general(jnp.concatenate([high, low], axis=0), kv[1, :, at], (((1,), (1,)), ((), ())),
                               preferred_element_type=jnp.float32)
        parts[s] = both[:8] + both[8:]
        totals[s] = carry

    later = jnp.zeros((8, HEAD), jnp.float32)
    total = jnp.zeros((8, HEAD), jnp.float32)
    for s in range(Z - 1, -1, -1):
        total = total + jnp.exp(later) * parts[s]
        later = later + totals[s, :, :HEAD]
    result[...] = total

    @pl.when(first)
    def _():
        remote(mbuf.at[z], columns, zs.at[LATER.index(0)], zr.at[sp], (z * 2 + 1, tp)).wait_send()

    for copy in sends:
        copy.wait_send()


def store(kv, result, keys, values, out, sems):
    copies = [pltpu.make_async_copy(kv.at[i], (keys, values)[i].at[0], sems.at[i]) for i in range(2)]
    for copy in copies:
        copy.start()
    out[0] = result[:2, :].astype(jnp.bfloat16)
    for copy in copies:
        copy.wait()


def local(prompt, input_gain, key_weight, value_weight, key_gain, queries, score_bias):
    hbm = pl.BlockSpec(memory_space=pltpu.HBM)
    vmem = pl.BlockSpec(memory_space=pltpu.VMEM)
    length = POS * 2 * Z
    dma = pltpu.SemaphoreType.DMA
    bf16 = jnp.bfloat16
    kv, result = pl.pallas_call(
        exchange,
        out_shape=(pltpu.VMEM((2, HEAD, length), bf16), pltpu.VMEM((8, HEAD), jnp.float32)),
        in_specs=[hbm, vmem, hbm, hbm, vmem, vmem, pl.BlockSpec(memory_space=pltpu.SMEM)],
        out_specs=(vmem, vmem),
        scratch_shapes=[
            pltpu.VMEM((POS, D), bf16),
            pltpu.VMEM((POS, D), bf16),
            pltpu.VMEM((16, UNIT, D), bf16),
            pltpu.VMEM((Z * UNIT, D), bf16),
            pltpu.VMEM((16, 2, HEAD, D), bf16),
            pltpu.VMEM((16, 2, HEAD, POS), bf16),
            pltpu.VMEM((16, 2, HEAD, POS), bf16),
            pltpu.VMEM((16, Z, UNIT, 2 * HEAD), bf16),
            pltpu.VMEM((Z, 2, 16, UNIT, 2 * HEAD), bf16),
            pltpu.VMEM((Z, 8, HEAD), jnp.float32),
            pltpu.VMEM((Z, 8, 128), jnp.float32),
            pltpu.SemaphoreType.REGULAR((8, 2)), dma((3,)), dma((15,)), dma((16,)), dma((16,)), dma((16,)), dma((6,)), dma((16,)), dma((16,)),
            dma((16,)), dma((16,)), dma((16,)), dma((16,)), dma((16,)), dma((32,)), dma((16,)), dma((32,)),
        ],
        compiler_params=pltpu.CompilerParams(collective_id=0, has_side_effects=True),
        name="exchange",
    )(prompt, input_gain.reshape(1, D), key_weight, value_weight, key_gain.reshape(1, HEAD),
      queries, score_bias)
    keys, values, out = pl.pallas_call(
        store,
        out_shape=(
            jax.ShapeDtypeStruct((1, HEAD, length), bf16),
            jax.ShapeDtypeStruct((1, HEAD, length), bf16),
            jax.ShapeDtypeStruct((1, 2, HEAD), bf16),
        ),
        in_specs=[vmem, vmem],
        out_specs=(hbm, hbm, vmem),
        scratch_shapes=[dma((2,))],
        name="store",
    )(pltpu.with_memory_space_constraint(kv, pltpu.VMEM), pltpu.with_memory_space_constraint(result, pltpu.VMEM))
    return keys, values, out


def solution(mesh):
    placed = (P("tp", "sp", None), P(), P("tp", None), P("tp", None), P(), P("sp", None, "tp"), P())
    return jax.shard_map(
        local,
        mesh=mesh,
        in_specs=placed,
        out_specs=(P("sp", "tp", None), P("sp", "tp", None), P("sp", None, "tp")),
        check_vma=False,
    )
```

```python
import jax
import jax.numpy as jnp
from jax import lax
from jax.experimental import pallas as pl
from jax.experimental.pallas import tpu as pltpu
from jax.sharding import PartitionSpec as P

HEAD = 64
EPS = 1e-06
MESH = pl.DeviceIdType.MESH
Y, X, Z = 4, 4, 16
POS = 256
D = 2048

ORDER = [(0, 0), (1, 0), (3, 0), (0, 1), (0, 3), (2, 0), (0, 2),
         (1, 1), (1, 3), (3, 1), (3, 3), (2, 1), (2, 3), (1, 2), (3, 2), (2, 2)]
SLOT = {offset: slot for slot, offset in enumerate(ORDER)}
UNIT = 16
STEPS = [8, 7, -7, 6, -6, 5, -5, 4, -4, 3, -3, 2, -2, 1, -1, 0]
LATER = [0, 8, 7, -7, 6, -6, 5, -5, 4, -4, 3, -3, 2, -2, 1, -1]
GROUPS = [(1, 5), (5, 7), (7, 11), (11, 15), (15, 16)]


def exchange(prompt, gain, kw, vw, kgain, queries, bias, kv, result, pbuf, nbuf, ubuf, xbuf, wbuf, sbuf, mbuf, ybuf, tbuf, parts, totals,
             tok, lsem, us, ur, bs, br, ws, wr, fs, ps, pr, ms, mr, zs, zr, ys, yr):
    sp = lax.axis_index("sp")
    tp = lax.axis_index("tp")
    z, c = sp // 2, lax.rem(sp, 2)
    y, x = tp // X, lax.rem(tp, X)
    first = c == 0
    partner = (z * 2 + 1 - c, tp)

    def plane(dy, dx):
        return lax.rem(y + dy + Y, Y) * X + lax.rem(x + dx + X, X)

    def remote(src, dst, send, recv, device):
        return pltpu.make_async_remote_copy(src_ref=src, dst_ref=dst, send_sem=send, recv_sem=recv,
                                            device_id=device, device_id_type=MESH)

    loads = [
        pltpu.make_async_copy(prompt.at[1], pbuf, lsem.at[0]),
        pltpu.make_async_copy(kw, wbuf.at[0, 0], lsem.at[1]),
        pltpu.make_async_copy(vw, wbuf.at[0, 1], lsem.at[2]),
    ]
    for load in loads:
        load.start()

    barrier = pltpu.get_barrier_semaphore()
    for dy, dx in ORDER[1:]:
        pl.semaphore_signal(barrier, inc=1, device_id=(sp, plane(dy, dx)), device_id_type=MESH)
    ahead = (lax.rem(sp + 2, 2 * Z), tp)
    behind = (lax.rem(sp + 2 * Z - 2, 2 * Z), tp)
    for device in (partner, ahead, behind):
        pl.semaphore_signal(barrier, inc=1, device_id=device, device_id_type=MESH)

    gain_row = gain[...]

    def norm(source, target):
        @pl.loop(0, POS // 32)
        def _(step):
            rows = pl.ds(pl.multiple_of(step * 32, 32), 32)
            flat = source[rows, :].astype(jnp.float32)
            scale = lax.rsqrt(jnp.mean(flat * flat, axis=-1, keepdims=True) + EPS)
            target[rows, :] = (flat * scale * gain_row).astype(jnp.bfloat16)

    pl.semaphore_wait(barrier, 15 + 3)

    sends, last = [], []

    def unit(j):
        return prompt.at[0, pl.ds(pl.multiple_of(j * UNIT, UNIT), UNIT), :]

    own = pltpu.make_async_copy(unit(tp), ubuf.at[tp], ur.at[tp])
    own.start()
    for slot, (dy, dx) in enumerate(ORDER[1:]):
        j = plane(dy, dx)
        copy = remote(unit(j), ubuf.at[tp], us.at[slot], ur.at[tp], (sp, j))
        copy.start()
        sends.append(copy)

    def send_weights():
        loads[1].wait()
        loads[2].wait()
        for i, offset in enumerate(ORDER[1:7]):
            copy = remote(wbuf.at[0, c], wbuf.at[SLOT[offset], c], ws.at[i], wr.at[SLOT[offset]],
                          (sp, plane(-offset[0], -offset[1])))
            copy.start()
            sends.append(copy)

    rows_here = xbuf.at[pl.ds(pl.multiple_of(z * UNIT, UNIT), UNIT), :]
    local_unit = None
    for i, hop in enumerate((1, 2, 4)):
        for side, d in enumerate((hop, -hop)):
            pl.semaphore_signal(tok.at[i, side], inc=1, device_id=(lax.rem(sp + 2 * d + 2 * Z, 2 * Z), tp),
                                device_id_type=MESH)
        for side in range(2):
            pl.semaphore_wait(tok.at[i, side], 1)
    send_weights()
    for i, d in enumerate(STEPS):
        t = lax.rem(z + d + Z, Z)
        pltpu.make_async_copy(ubuf.at[t], ubuf.at[t], ur.at[t]).wait()
        if d == 0:
            local_unit = pltpu.make_async_copy(ubuf.at[t], rows_here, bs.at[i])
            local_unit.start()
        else:
            copy = remote(ubuf.at[t], rows_here, bs.at[i], br.at[z], (t * 2 + c, tp))
            copy.start()
            sends.append(copy)

    loads[0].wait()
    norm(pbuf, nbuf)

    eye = lax.broadcasted_iota(jnp.int32, (HEAD, HEAD), 0) == lax.broadcasted_iota(jnp.int32, (HEAD, HEAD), 1)
    gain_col = jnp.sum(jnp.where(eye, kgain[...], 0.0), axis=1, keepdims=True)

    def project(lo, hi):
        count = hi - lo
        weights = wbuf[lo:hi].reshape(count * 2 * HEAD, D)
        raw = lax.dot_general(weights, nbuf[...], (((1,), (1,)), ((), ())), preferred_element_type=jnp.float32)
        for i in range(count):
            key = raw[i * 2 * HEAD: i * 2 * HEAD + HEAD]
            scale = lax.rsqrt(jnp.mean(key * key, axis=0, keepdims=True) + EPS)
            sbuf[lo + i, 0] = (key * scale * gain_col).astype(jnp.bfloat16)
            sbuf[lo + i, 1] = raw[i * 2 * HEAD + HEAD: (i + 1) * 2 * HEAD].astype(jnp.bfloat16)

    def arrive(slot):
        half = remote(wbuf.at[slot, c], wbuf.at[slot, c], ps.at[slot], wr.at[slot], partner)
        half.wait_recv()
        over = remote(wbuf.at[slot, c], wbuf.at[slot, c], ps.at[slot], pr.at[slot], partner)
        over.start()
        sends.append(over)

    def other(slot):
        remote(wbuf.at[slot, 1 - c], wbuf.at[slot, 1 - c], ps.at[slot], pr.at[slot], partner).wait_recv()

    def spread(step):
        source = jnp.where(first, SLOT[(step, 0)], SLOT[(0, step)])
        for hop in (1, 3, 2):
            slot = jnp.where(first, SLOT[(step, hop)], SLOT[(hop, step)])
            target = jnp.where(first, plane(0, -hop), plane(-hop, 0))
            copy = remote(wbuf.at[source, c], wbuf.at[slot, c], fs.at[step * 4 + hop], wr.at[slot], (sp, target))
            copy.start()
            sends.append(copy)

    def hand(slot):
        dy, dx = ORDER[slot]
        if slot == 0:
            pltpu.make_async_copy(sbuf.at[slot], mbuf.at[tp], mr.at[tp]).start()
        else:
            copy = remote(sbuf.at[slot], mbuf.at[tp], ms.at[slot], mr.at[tp], (sp, plane(dy, dx)))
            copy.start()
            sends.append(copy)

    project(0, 1)
    hand(0)
    for number, (lo, hi) in enumerate(GROUPS):
        for slot in range(lo, hi):
            arrive(slot)
        if number == 0:
            spread(1)
            spread(3)
        if number == 1:
            spread(2)
        for slot in range(lo, hi):
            other(slot)
        project(lo, hi)
        for slot in range(lo, hi):
            hand(slot)

    columns = kv.at[:, :, pl.ds(pl.multiple_of(sp * POS, POS), POS)]
    for i, d in enumerate(LATER):
        t = lax.rem(z + d + Z, Z)
        pltpu.make_async_copy(mbuf.at[t], mbuf.at[t], mr.at[t]).wait()
        far = remote(mbuf.at[t], columns, zs.at[i], zr.at[sp], (t * 2 + 1, tp))
        if d == 0:
            near = pltpu.make_async_copy(mbuf.at[t], columns, zs.at[i])

            @pl.when(first)
            def _():
                far.start()

            @pl.when(jnp.logical_not(first))
            def _():
                near.start()
        else:
            far.start()
            last.append(far)

    local_unit.wait()
    for d in STEPS:
        if d != 0:
            s = lax.rem(z + d + Z, Z)
            came = xbuf.at[pl.ds(pl.multiple_of(s * UNIT, UNIT), UNIT), :]
            remote(came, came, bs.at[0], br.at[s], partner).wait_recv()

    norm(xbuf, xbuf)
    lane = lax.broadcasted_iota(jnp.int32, (1, 2 * HEAD), 1)
    gain_both = jnp.concatenate([kgain[...], kgain[...]], axis=1)
    place = tbuf.at[:, c, tp]
    for slot, (dy, dx) in enumerate(ORDER):
        weights = wbuf[slot].reshape(2 * HEAD, D)
        raw = lax.dot_general(xbuf[...], weights, (((1,), (1,)), ((), ())), preferred_element_type=jnp.float32)
        mean = jnp.sum(jnp.where(lane < HEAD, raw * raw, 0.0), axis=1, keepdims=True) * (1.0 / HEAD)
        scale = jnp.where(lane < HEAD, lax.rsqrt(mean + EPS) * gain_both, 1.0)
        ybuf[slot] = (raw * scale).astype(jnp.bfloat16).reshape(Z, UNIT, 2 * HEAD)
        far = remote(ybuf.at[slot], place, ys.at[slot], yr.at[tp * 2 + c], (z * 2, plane(dy, dx)))
        if slot == 0:
            near_y = pltpu.make_async_copy(ybuf.at[slot], place, ys.at[slot])
            far_y = far

            @pl.when(first)
            def _():
                near_y.start()

            @pl.when(jnp.logical_not(first))
            def _():
                far_y.start()
        else:
            far.start()
            sends.append(far)

    @pl.when(first)
    def _():
        near_y.wait()

        @pl.loop(0, 2 * 16)
        def _(source):
            @pl.when(source != tp * 2)
            def _():
                came = tbuf.at[:, lax.rem(source, 2), source // 2]
                remote(came, came, ys.at[0], yr.at[source], partner).wait_recv()

        one = lax.broadcasted_iota(jnp.int32, (128, 128), 0) == lax.broadcasted_iota(jnp.int32, (128, 128), 1)
        identity = jnp.where(one, 1.0, 0.0).astype(jnp.bfloat16)

        @pl.loop(0, 2 * Z)
        def _(p):
            rows = tbuf[p // 2, lax.rem(p, 2)].reshape(POS, 2 * HEAD)
            turned = lax.dot_general(identity, rows, (((1,), (1,)), ((), ())), preferred_element_type=jnp.float32)
            turned = turned.astype(jnp.bfloat16)
            span = pl.ds(pl.multiple_of(p * POS, POS), POS)
            kv[0, :, span] = turned[:HEAD]
            kv[1, :, span] = turned[HEAD:]

    @pl.when(jnp.logical_not(first))
    def _():
        far_y.wait_send()
        pltpu.make_async_copy(mbuf.at[z], columns, zs.at[LATER.index(0)]).wait()

    for copy in sends:
        copy.wait_send()

    q = jnp.concatenate([queries[0], jnp.zeros((6, HEAD), jnp.bfloat16)], axis=0)
    row = lax.broadcasted_iota(jnp.int32, (8, 1), 0)
    offset = jnp.where(row == 0, bias[0, tp], bias[1, tp])
    r = lax.broadcasted_iota(jnp.int32, (128, 256), 0)
    col = lax.broadcasted_iota(jnp.int32, (128, 256), 1)
    tri = jnp.where((r > col) | (col >= 128), 1.0, 0.0).astype(jnp.bfloat16)
    span = 2 * POS

    @pl.loop(0, Z)
    def _(i):
        far_by = Z // 2 - i // 2
        d = jnp.where(i == 0, 0, jnp.where(lax.rem(i, 2) == 0, far_by, -far_by))
        s = lax.rem(z - d + Z, Z)

        @pl.when(jnp.logical_not(first))
        def _():
            for core in range(2):
                p = s * 2 + core

                @pl.when(p != sp)
                def _():
                    came = kv.at[:, :, pl.ds(pl.multiple_of(p * POS, POS), POS)]
                    remote(came, came, zs.at[0], zr.at[p], partner).wait_recv()

        at = pl.ds(pl.multiple_of(s * span, span), span)
        scores = jnp.dot(q, kv[0, :, at], preferred_element_type=jnp.float32) * 0.125 + offset
        soft = jnp.log1p(jnp.exp(-jnp.abs(scores)))
        log_break = jnp.minimum(scores, 0.0) - soft
        log_keep = jnp.minimum(-scores, 0.0) - soft
        stacked = jnp.concatenate([log_keep[:, b * 128:(b + 1) * 128] for b in range(span // 128)], axis=0)
        thirds = []
        for _ in range(3):
            thirds.append(stacked.astype(jnp.bfloat16))
            stacked = stacked - thirds[-1].astype(jnp.float32)
        rows = 8 * (span // 128)
        sums = jnp.dot(jnp.concatenate(thirds, axis=0), tri, preferred_element_type=jnp.float32)
        sums = (sums[2 * rows:] + sums[rows:2 * rows]) + sums[:rows]
        carry = jnp.zeros((8, 128), jnp.float32)
        pieces = [None] * (span // 128)
        for b in range(span // 128 - 1, -1, -1):
            pieces[b] = sums[b * 8:(b + 1) * 8, :128] + carry
            carry = carry + sums[b * 8:(b + 1) * 8, 128:]
        weights = jnp.exp(log_break + jnp.concatenate(pieces, axis=1))
        high = weights.astype(jnp.bfloat16)
        low = (weights - high.astype(jnp.float32)).astype(jnp.bfloat16)
        both = lax.dot_general(jnp.concatenate([high, low], axis=0), kv[1, :, at], (((1,), (1,)), ((), ())),
                               preferred_element_type=jnp.float32)
        parts[s] = both[:8] + both[8:]
        totals[s] = carry

    later = jnp.zeros((8, HEAD), jnp.float32)
    total = jnp.zeros((8, HEAD), jnp.float32)
    for s in range(Z - 1, -1, -1):
        total = total + jnp.exp(later) * parts[s]
        later = later + totals[s, :, :HEAD]
    result[...] = total

    @pl.when(first)
    def _():
        remote(mbuf.at[z], columns, zs.at[LATER.index(0)], zr.at[sp], (z * 2 + 1, tp)).wait_send()

    for copy in last:
        copy.wait_send()


def store(kv, result, keys, values, out, sems):
    copies = [pltpu.make_async_copy(kv.at[i], (keys, values)[i].at[0], sems.at[i]) for i in range(2)]
    for copy in copies:
        copy.start()
    out[0] = result[:2, :].astype(jnp.bfloat16)
    for copy in copies:
        copy.wait()


def local(prompt, input_gain, key_weight, value_weight, key_gain, queries, score_bias):
    hbm = pl.BlockSpec(memory_space=pltpu.HBM)
    vmem = pl.BlockSpec(memory_space=pltpu.VMEM)
    length = POS * 2 * Z
    dma = pltpu.SemaphoreType.DMA
    bf16 = jnp.bfloat16
    kv, result = pl.pallas_call(
        exchange,
        out_shape=(pltpu.VMEM((2, HEAD, length), bf16), pltpu.VMEM((8, HEAD), jnp.float32)),
        in_specs=[hbm, vmem, hbm, hbm, vmem, vmem, pl.BlockSpec(memory_space=pltpu.SMEM)],
        out_specs=(vmem, vmem),
        scratch_shapes=[
            pltpu.VMEM((POS, D), bf16),
            pltpu.VMEM((POS, D), bf16),
            pltpu.VMEM((16, UNIT, D), bf16),
            pltpu.VMEM((Z * UNIT, D), bf16),
            pltpu.VMEM((16, 2, HEAD, D), bf16),
            pltpu.VMEM((16, 2, HEAD, POS), bf16),
            pltpu.VMEM((16, 2, HEAD, POS), bf16),
            pltpu.VMEM((16, Z, UNIT, 2 * HEAD), bf16),
            pltpu.VMEM((Z, 2, 16, UNIT, 2 * HEAD), bf16),
            pltpu.VMEM((Z, 8, HEAD), jnp.float32),
            pltpu.VMEM((Z, 8, 128), jnp.float32),
            pltpu.SemaphoreType.REGULAR((8, 2)), dma((3,)), dma((15,)), dma((16,)), dma((16,)), dma((16,)), dma((6,)), dma((16,)), dma((16,)),
            dma((16,)), dma((16,)), dma((16,)), dma((16,)), dma((16,)), dma((32,)), dma((16,)), dma((32,)),
        ],
        compiler_params=pltpu.CompilerParams(collective_id=0, has_side_effects=True),
        name="exchange",
    )(prompt, input_gain.reshape(1, D), key_weight, value_weight, key_gain.reshape(1, HEAD),
      queries, score_bias)
    keys, values, out = pl.pallas_call(
        store,
        out_shape=(
            jax.ShapeDtypeStruct((1, HEAD, length), bf16),
            jax.ShapeDtypeStruct((1, HEAD, length), bf16),
            jax.ShapeDtypeStruct((1, 2, HEAD), bf16),
        ),
        in_specs=[vmem, vmem],
        out_specs=(hbm, hbm, vmem),
        scratch_shapes=[dma((2,))],
        name="store",
    )(pltpu.with_memory_space_constraint(kv, pltpu.VMEM), pltpu.with_memory_space_constraint(result, pltpu.VMEM))
    return keys, values, out


def solution(mesh):
    placed = (P("tp", "sp", None), P(), P("tp", None), P("tp", None), P(), P("sp", None, "tp"), P())
    return jax.shard_map(
        local,
        mesh=mesh,
        in_specs=placed,
        out_specs=(P("sp", "tp", None), P("sp", "tp", None), P("sp", None, "tp")),
        check_vma=False,
    )
```

```python
import jax
import jax.numpy as jnp
from jax import lax
from jax.experimental import pallas as pl
from jax.experimental.pallas import tpu as pltpu
from jax.sharding import PartitionSpec as P

HEAD = 64
EPS = 1e-06
MESH = pl.DeviceIdType.MESH
Y, X, Z = 4, 4, 16
POS = 256
D = 2048

ORDER = [(0, 0), (1, 0), (3, 0), (0, 1), (0, 3), (2, 0), (0, 2),
         (1, 1), (1, 3), (3, 1), (3, 3), (2, 1), (2, 3), (1, 2), (3, 2), (2, 2)]
SLOT = {offset: slot for slot, offset in enumerate(ORDER)}
UNIT = 16
STEPS = [8, 7, -7, 6, -6, 5, -5, 4, -4, 3, -3, 2, -2, 1, -1, 0]
LATER = [0, 8, 7, -7, 6, -6, 5, -5, 4, -4, 3, -3, 2, -2, 1, -1]
GROUPS = [(1, 5), (5, 7), (7, 11), (11, 15), (15, 16)]


def exchange(prompt, gain, kw, vw, kgain, queries, bias, kv, result, pbuf, nbuf, ubuf, xbuf, wbuf, sbuf, mbuf, ybuf, tbuf, parts, totals,
             tok, lsem, us, ur, bs, br, ws, wr, fs, ps, pr, ms, mr, zs, zr, ys, yr):
    sp = lax.axis_index("sp")
    tp = lax.axis_index("tp")
    z, c = sp // 2, lax.rem(sp, 2)
    y, x = tp // X, lax.rem(tp, X)
    first = c == 0
    partner = (z * 2 + 1 - c, tp)

    def plane(dy, dx):
        return lax.rem(y + dy + Y, Y) * X + lax.rem(x + dx + X, X)

    def remote(src, dst, send, recv, device):
        return pltpu.make_async_remote_copy(src_ref=src, dst_ref=dst, send_sem=send, recv_sem=recv,
                                            device_id=device, device_id_type=MESH)

    loads = [
        pltpu.make_async_copy(prompt.at[1], pbuf, lsem.at[0]),
        pltpu.make_async_copy(kw, wbuf.at[0, 0], lsem.at[1]),
        pltpu.make_async_copy(vw, wbuf.at[0, 1], lsem.at[2]),
    ]
    for load in loads:
        load.start()

    barrier = pltpu.get_barrier_semaphore()
    for dy, dx in ORDER[1:]:
        pl.semaphore_signal(barrier, inc=1, device_id=(sp, plane(dy, dx)), device_id_type=MESH)
    ahead = (lax.rem(sp + 2, 2 * Z), tp)
    behind = (lax.rem(sp + 2 * Z - 2, 2 * Z), tp)
    for device in (partner, ahead, behind):
        pl.semaphore_signal(barrier, inc=1, device_id=device, device_id_type=MESH)

    gain_row = gain[...]

    def norm(source, target):
        @pl.loop(0, POS // 32)
        def _(step):
            rows = pl.ds(pl.multiple_of(step * 32, 32), 32)
            flat = source[rows, :].astype(jnp.float32)
            scale = lax.rsqrt(jnp.mean(flat * flat, axis=-1, keepdims=True) + EPS)
            target[rows, :] = (flat * scale * gain_row).astype(jnp.bfloat16)

    def tell(i, hop):
        for side, d in enumerate((hop, -hop)):
            pl.semaphore_signal(tok.at[i, side], inc=1, device_id=(lax.rem(sp + 2 * d + 2 * Z, 2 * Z), tp),
                                device_id_type=MESH)

    pl.semaphore_wait(barrier, 15 + 3)
    tell(0, 1)

    sends, last = [], []

    def unit(j):
        return prompt.at[0, pl.ds(pl.multiple_of(j * UNIT, UNIT), UNIT), :]

    own = pltpu.make_async_copy(unit(tp), ubuf.at[tp], ur.at[tp])
    own.start()
    for slot, (dy, dx) in enumerate(ORDER[1:]):
        j = plane(dy, dx)
        copy = remote(unit(j), ubuf.at[tp], us.at[slot], ur.at[tp], (sp, j))
        copy.start()
        sends.append(copy)

    def send_weights():
        loads[1].wait()
        loads[2].wait()
        for i, offset in enumerate(ORDER[1:7]):
            copy = remote(wbuf.at[0, c], wbuf.at[SLOT[offset], c], ws.at[i], wr.at[SLOT[offset]],
                          (sp, plane(-offset[0], -offset[1])))
            copy.start()
            sends.append(copy)

    rows_here = xbuf.at[pl.ds(pl.multiple_of(z * UNIT, UNIT), UNIT), :]
    local_unit = None
    for i, hop in enumerate((1, 2, 4)):
        if hop > 1:
            tell(i, hop)
        for side in range(2):
            pl.semaphore_wait(tok.at[i, side], 1)
    send_weights()
    for i, d in enumerate(STEPS):
        t = lax.rem(z + d + Z, Z)
        pltpu.make_async_copy(ubuf.at[t], ubuf.at[t], ur.at[t]).wait()
        if d == 0:
            local_unit = pltpu.make_async_copy(ubuf.at[t], rows_here, bs.at[i])
            local_unit.start()
        else:
            copy = remote(ubuf.at[t], rows_here, bs.at[i], br.at[z], (t * 2 + c, tp))
            copy.start()
            sends.append(copy)

    loads[0].wait()
    norm(pbuf, nbuf)

    eye = lax.broadcasted_iota(jnp.int32, (HEAD, HEAD), 0) == lax.broadcasted_iota(jnp.int32, (HEAD, HEAD), 1)
    gain_col = jnp.sum(jnp.where(eye, kgain[...], 0.0), axis=1, keepdims=True)

    def project(lo, hi):
        count = hi - lo
        weights = wbuf[lo:hi].reshape(count * 2 * HEAD, D)
        raw = lax.dot_general(weights, nbuf[...], (((1,), (1,)), ((), ())), preferred_element_type=jnp.float32)
        for i in range(count):
            key = raw[i * 2 * HEAD: i * 2 * HEAD + HEAD]
            scale = lax.rsqrt(jnp.mean(key * key, axis=0, keepdims=True) + EPS)
            sbuf[lo + i, 0] = (key * scale * gain_col).astype(jnp.bfloat16)
            sbuf[lo + i, 1] = raw[i * 2 * HEAD + HEAD: (i + 1) * 2 * HEAD].astype(jnp.bfloat16)

    def arrive(slot):
        half = remote(wbuf.at[slot, c], wbuf.at[slot, c], ps.at[slot], wr.at[slot], partner)
        half.wait_recv()
        over = remote(wbuf.at[slot, c], wbuf.at[slot, c], ps.at[slot], pr.at[slot], partner)
        over.start()
        sends.append(over)

    def other(slot):
        remote(wbuf.at[slot, 1 - c], wbuf.at[slot, 1 - c], ps.at[slot], pr.at[slot], partner).wait_recv()

    def spread(step):
        source = jnp.where(first, SLOT[(step, 0)], SLOT[(0, step)])
        for hop in (1, 3, 2):
            slot = jnp.where(first, SLOT[(step, hop)], SLOT[(hop, step)])
            target = jnp.where(first, plane(0, -hop), plane(-hop, 0))
            copy = remote(wbuf.at[source, c], wbuf.at[slot, c], fs.at[step * 4 + hop], wr.at[slot], (sp, target))
            copy.start()
            sends.append(copy)

    def hand(slot):
        dy, dx = ORDER[slot]
        if slot == 0:
            pltpu.make_async_copy(sbuf.at[slot], mbuf.at[tp], mr.at[tp]).start()
        else:
            copy = remote(sbuf.at[slot], mbuf.at[tp], ms.at[slot], mr.at[tp], (sp, plane(dy, dx)))
            copy.start()
            sends.append(copy)

    project(0, 1)
    hand(0)
    for number, (lo, hi) in enumerate(GROUPS):
        for slot in range(lo, hi):
            arrive(slot)
        if number == 0:
            spread(1)
            spread(3)
        if number == 1:
            spread(2)
        for slot in range(lo, hi):
            other(slot)
        project(lo, hi)
        for slot in range(lo, hi):
            hand(slot)

    columns = kv.at[:, :, pl.ds(pl.multiple_of(sp * POS, POS), POS)]
    for i, d in enumerate(LATER):
        t = lax.rem(z + d + Z, Z)
        pltpu.make_async_copy(mbuf.at[t], mbuf.at[t], mr.at[t]).wait()
        far = remote(mbuf.at[t], columns, zs.at[i], zr.at[sp], (t * 2 + 1, tp))
        if d == 0:
            near = pltpu.make_async_copy(mbuf.at[t], columns, zs.at[i])

            @pl.when(first)
            def _():
                far.start()

            @pl.when(jnp.logical_not(first))
            def _():
                near.start()
        else:
            far.start()
            last.append(far)

    local_unit.wait()
    for d in STEPS:
        if d != 0:
            s = lax.rem(z + d + Z, Z)
            came = xbuf.at[pl.ds(pl.multiple_of(s * UNIT, UNIT), UNIT), :]
            remote(came, came, bs.at[0], br.at[s], partner).wait_recv()

    norm(xbuf, xbuf)
    lane = lax.broadcasted_iota(jnp.int32, (1, 2 * HEAD), 1)
    gain_both = jnp.concatenate([kgain[...], kgain[...]], axis=1)
    place = tbuf.at[:, c, tp]
    for slot, (dy, dx) in enumerate(ORDER):
        weights = wbuf[slot].reshape(2 * HEAD, D)
        raw = lax.dot_general(xbuf[...], weights, (((1,), (1,)), ((), ())), preferred_element_type=jnp.float32)
        mean = jnp.sum(jnp.where(lane < HEAD, raw * raw, 0.0), axis=1, keepdims=True) * (1.0 / HEAD)
        scale = jnp.where(lane < HEAD, lax.rsqrt(mean + EPS) * gain_both, 1.0)
        ybuf[slot] = (raw * scale).astype(jnp.bfloat16).reshape(Z, UNIT, 2 * HEAD)
        far = remote(ybuf.at[slot], place, ys.at[slot], yr.at[tp * 2 + c], (z * 2, plane(dy, dx)))
        if slot == 0:
            near_y = pltpu.make_async_copy(ybuf.at[slot], place, ys.at[slot])
            far_y = far

            @pl.when(first)
            def _():
                near_y.start()

            @pl.when(jnp.logical_not(first))
            def _():
                far_y.start()
        else:
            far.start()
            sends.append(far)

    @pl.when(first)
    def _():
        near_y.wait()

        @pl.loop(0, 2 * 16)
        def _(source):
            @pl.when(source != tp * 2)
            def _():
                came = tbuf.at[:, lax.rem(source, 2), source // 2]
                remote(came, came, ys.at[0], yr.at[source], partner).wait_recv()

        one = lax.broadcasted_iota(jnp.int32, (128, 128), 0) == lax.broadcasted_iota(jnp.int32, (128, 128), 1)
        identity = jnp.where(one, 1.0, 0.0).astype(jnp.bfloat16)

        @pl.loop(0, 2 * Z)
        def _(p):
            rows = tbuf[p // 2, lax.rem(p, 2)].reshape(POS, 2 * HEAD)
            turned = lax.dot_general(identity, rows, (((1,), (1,)), ((), ())), preferred_element_type=jnp.float32)
            turned = turned.astype(jnp.bfloat16)
            span = pl.ds(pl.multiple_of(p * POS, POS), POS)
            kv[0, :, span] = turned[:HEAD]
            kv[1, :, span] = turned[HEAD:]

    @pl.when(jnp.logical_not(first))
    def _():
        far_y.wait_send()
        pltpu.make_async_copy(mbuf.at[z], columns, zs.at[LATER.index(0)]).wait()

    for copy in sends:
        copy.wait_send()

    q = jnp.concatenate([queries[0], jnp.zeros((6, HEAD), jnp.bfloat16)], axis=0)
    row = lax.broadcasted_iota(jnp.int32, (8, 1), 0)
    offset = jnp.where(row == 0, bias[0, tp], bias[1, tp])
    r = lax.broadcasted_iota(jnp.int32, (128, 256), 0)
    col = lax.broadcasted_iota(jnp.int32, (128, 256), 1)
    tri = jnp.where((r > col) | (col >= 128), 1.0, 0.0).astype(jnp.bfloat16)
    span = 2 * POS

    @pl.loop(0, Z)
    def _(i):
        far_by = Z // 2 - i // 2
        d = jnp.where(i == 0, 0, jnp.where(lax.rem(i, 2) == 0, far_by, -far_by))
        s = lax.rem(z - d + Z, Z)

        @pl.when(jnp.logical_not(first))
        def _():
            for core in range(2):
                p = s * 2 + core

                @pl.when(p != sp)
                def _():
                    came = kv.at[:, :, pl.ds(pl.multiple_of(p * POS, POS), POS)]
                    remote(came, came, zs.at[0], zr.at[p], partner).wait_recv()

        at = pl.ds(pl.multiple_of(s * span, span), span)
        scores = jnp.dot(q, kv[0, :, at], preferred_element_type=jnp.float32) * 0.125 + offset
        soft = jnp.log1p(jnp.exp(-jnp.abs(scores)))
        log_break = jnp.minimum(scores, 0.0) - soft
        log_keep = jnp.minimum(-scores, 0.0) - soft
        stacked = jnp.concatenate([log_keep[:, b * 128:(b + 1) * 128] for b in range(span // 128)], axis=0)
        thirds = []
        for _ in range(3):
            thirds.append(stacked.astype(jnp.bfloat16))
            stacked = stacked - thirds[-1].astype(jnp.float32)
        rows = 8 * (span // 128)
        sums = jnp.dot(jnp.concatenate(thirds, axis=0), tri, preferred_element_type=jnp.float32)
        sums = (sums[2 * rows:] + sums[rows:2 * rows]) + sums[:rows]
        carry = jnp.zeros((8, 128), jnp.float32)
        pieces = [None] * (span // 128)
        for b in range(span // 128 - 1, -1, -1):
            pieces[b] = sums[b * 8:(b + 1) * 8, :128] + carry
            carry = carry + sums[b * 8:(b + 1) * 8, 128:]
        weights = jnp.exp(log_break + jnp.concatenate(pieces, axis=1))
        high = weights.astype(jnp.bfloat16)
        low = (weights - high.astype(jnp.float32)).astype(jnp.bfloat16)
        both = lax.dot_general(jnp.concatenate([high, low], axis=0), kv[1, :, at], (((1,), (1,)), ((), ())),
                               preferred_element_type=jnp.float32)
        parts[s] = both[:8] + both[8:]
        totals[s] = carry

    later = jnp.zeros((8, HEAD), jnp.float32)
    total = jnp.zeros((8, HEAD), jnp.float32)
    for s in range(Z - 1, -1, -1):
        total = total + jnp.exp(later) * parts[s]
        later = later + totals[s, :, :HEAD]
    result[...] = total

    @pl.when(first)
    def _():
        remote(mbuf.at[z], columns, zs.at[LATER.index(0)], zr.at[sp], (z * 2 + 1, tp)).wait_send()

    for copy in last:
        copy.wait_send()


def store(kv, result, keys, values, out, sems):
    copies = [pltpu.make_async_copy(kv.at[i], (keys, values)[i].at[0], sems.at[i]) for i in range(2)]
    for copy in copies:
        copy.start()
    out[0] = result[:2, :].astype(jnp.bfloat16)
    for copy in copies:
        copy.wait()


def local(prompt, input_gain, key_weight, value_weight, key_gain, queries, score_bias):
    hbm = pl.BlockSpec(memory_space=pltpu.HBM)
    vmem = pl.BlockSpec(memory_space=pltpu.VMEM)
    length = POS * 2 * Z
    dma = pltpu.SemaphoreType.DMA
    bf16 = jnp.bfloat16
    kv, result = pl.pallas_call(
        exchange,
        out_shape=(pltpu.VMEM((2, HEAD, length), bf16), pltpu.VMEM((8, HEAD), jnp.float32)),
        in_specs=[hbm, vmem, hbm, hbm, vmem, vmem, pl.BlockSpec(memory_space=pltpu.SMEM)],
        out_specs=(vmem, vmem),
        scratch_shapes=[
            pltpu.VMEM((POS, D), bf16),
            pltpu.VMEM((POS, D), bf16),
            pltpu.VMEM((16, UNIT, D), bf16),
            pltpu.VMEM((Z * UNIT, D), bf16),
            pltpu.VMEM((16, 2, HEAD, D), bf16),
            pltpu.VMEM((16, 2, HEAD, POS), bf16),
            pltpu.VMEM((16, 2, HEAD, POS), bf16),
            pltpu.VMEM((16, Z, UNIT, 2 * HEAD), bf16),
            pltpu.VMEM((Z, 2, 16, UNIT, 2 * HEAD), bf16),
            pltpu.VMEM((Z, 8, HEAD), jnp.float32),
            pltpu.VMEM((Z, 8, 128), jnp.float32),
            pltpu.SemaphoreType.REGULAR((8, 2)), dma((3,)), dma((15,)), dma((16,)), dma((16,)), dma((16,)), dma((6,)), dma((16,)), dma((16,)),
            dma((16,)), dma((16,)), dma((16,)), dma((16,)), dma((16,)), dma((32,)), dma((16,)), dma((32,)),
        ],
        compiler_params=pltpu.CompilerParams(collective_id=0, has_side_effects=True),
        name="exchange",
    )(prompt, input_gain.reshape(1, D), key_weight, value_weight, key_gain.reshape(1, HEAD),
      queries, score_bias)
    keys, values, out = pl.pallas_call(
        store,
        out_shape=(
            jax.ShapeDtypeStruct((1, HEAD, length), bf16),
            jax.ShapeDtypeStruct((1, HEAD, length), bf16),
            jax.ShapeDtypeStruct((1, 2, HEAD), bf16),
        ),
        in_specs=[vmem, vmem],
        out_specs=(hbm, hbm, vmem),
        scratch_shapes=[dma((2,))],
        name="store",
    )(pltpu.with_memory_space_constraint(kv, pltpu.VMEM), pltpu.with_memory_space_constraint(result, pltpu.VMEM))
    return keys, values, out


def solution(mesh):
    placed = (P("tp", "sp", None), P(), P("tp", None), P("tp", None), P(), P("sp", None, "tp"), P())
    return jax.shard_map(
        local,
        mesh=mesh,
        in_specs=placed,
        out_specs=(P("sp", "tp", None), P("sp", "tp", None), P("sp", None, "tp")),
        check_vma=False,
    )
```
